32 devices in a mesh: ep: 16 (over z, y, x), tp: 2 (over core).
Axes of the slice: x: 2, y: 2, z: 4, core: 2. Of those that a mesh axis runs over, the one named last changes fastest.
Arguments:
- tokens: bfloat16 [256, 2048], P('ep'), may hold values from -6 to 6
- cache_keys: bfloat16 [256, 2, 64, 1024], P('ep', 'tp'), may hold values from -6 to 6
- cache_values: bfloat16 [256, 2, 64, 1024], P('ep', 'tp'), may hold values from -6 to 6
- cache_lengths: int32 [256], P('ep'), may hold values from 1 to 1024, as said below
- norm_in: float32 [2048], replicated, may hold values from 0.1 to 1.9
- w_query: bfloat16 [2048, 512], P(None, 'tp'), may hold values from -0.125 to 0.125
- w_key: bfloat16 [2048, 128], P(None, 'tp'), may hold values from -0.125 to 0.125
- w_value: bfloat16 [2048, 128], P(None, 'tp'), may hold values from -0.125 to 0.125
- stick_bias: float32 [8], P('tp'), may hold values from -8 to -1.5
- w_output: bfloat16 [512, 2048], P('tp'), may hold values from -0.75 to 0.75
- norm_mid: float32 [2048], replicated, may hold values from 0.1 to 1.9
- routes: int32 [256, 6], P('ep'), may hold values from 0 to 15, all different within a row; in each aligned block of 16 rows (0 to 15, 16 to 31, ...) at most 6 rows name the same one
- route_weights: float32 [256, 6], P('ep'), may hold values from 0.1 to 1
- expert_gate: bfloat16 [16, 2048, 512], P('ep', None, 'tp'), may hold values from -0.125 to 0.125
- expert_up: bfloat16 [16, 2048, 512], P('ep', None, 'tp'), may hold values from -0.125 to 0.125
- expert_down: bfloat16 [16, 512, 2048], P('ep', 'tp'), may hold values from -0.25 to 0.25
- dense_gate: bfloat16 [2048, 256], P('ep'), may hold values from -0.125 to 0.125
- dense_up: bfloat16 [2048, 256], P('ep'), may hold values from -0.125 to 0.125
- dense_down: bfloat16 [256, 2048], P(None, 'ep'), may hold values from -0.375 to 0.375
- mix_gate: float32 [2048], replicated, may hold values from -0.125 to 0.125
- norm_out: float32 [2048], replicated, may hold values from 0.1 to 1.9
Outputs:
- mixed: bfloat16 [256, 2048], P('ep')
- fresh_keys: bfloat16 [256, 128], P('ep', 'tp')
- fresh_values: bfloat16 [256, 128], P('ep', 'tp')
The draws below stay inside these ranges and needn't reach their ends.
Inputs may be any that keep to these rules, and one draw needn't show every extreme that they name: `cache_lengths`: positions at or past a sequence's length are not read. Among the sequences of one index of ep some sequence has length 1024. `routes`: each row names 6 different experts; among the rows of one index of ep (aligned blocks of 16 rows) no expert is named by more than 6 rows, and that bound is reached.
All inputs are finite; a program needn't handle non-finite values.
Results may differ from the reference program's by a relative error of at most 0.015.
Values may be sent and summed in bfloat16 or wider, within the bound.
No kernel may reach another device: no remote copies, remote signals or barrier semaphores. Data moves between devices by JAX's collectives and lax.ppermute only.
A program may use at most 64 MiB of HBM per device.

```python
import math
import jax
import jax.numpy as jnp
import numpy as np
from jax import lax

D = 2048
HEADS = 8
KVH = 2
HD = 64
EW = 512
SHARED = 256
TOPK = 6
SEQ_DEV = 16
CACHE = 1024
SEQS = 256
EXPERTS = 16
CAP = 6
N_EP = 16
N_TP = 2


def draw_cache_lengths(key, part):
    first_key, second_key = jax.random.split(jax.random.fold_in(key, 11))
    drawn_lengths = jax.random.randint(first_key, (SEQS,), 1, CACHE + 1)
    chosen = jax.random.randint(second_key, (SEQS // SEQ_DEV,), 0, SEQ_DEV)
    position = jnp.arange(SEQS)
    is_full = position % SEQ_DEV == jnp.repeat(chosen, SEQ_DEV)
    return jnp.where(is_full, CACHE, drawn_lengths).astype(jnp.int32)


def draw_stick_bias(key, part):
    first_key, second_key, third_key = jax.random.split(jax.random.fold_in(key, 23), 3)
    is_fast = jax.random.randint(first_key, (HEADS,), 0, 2) == 1
    fast_bias = jax.random.uniform(second_key, (HEADS,), jnp.float32, -2.5, -1.5)
    slow_bias = jax.random.uniform(third_key, (HEADS,), jnp.float32, -7.5, -6.0)
    return jnp.where(is_fast, fast_bias, slow_bias).astype(jnp.float32)


def shard_levels(rng, shape, cuts, least, largest):
    loudness, own = 1.0, jax.random.fold_in(rng, 6)
    for dim, shards_of in cuts:
        draws = jnp.exp(jax.random.uniform(jax.random.fold_in(own, dim), (shards_of,), jnp.float32, least / len(cuts), largest / len(cuts)))
        loudness = loudness * jnp.repeat(draws, shape[dim] // shards_of).reshape([-1 if axis == dim else 1 for axis in range(len(shape))])
    return loudness


def deal_out(rng, own, number, rows, amount, top, most, slope):
    sequence = jax.random.permutation(rng, amount)
    packed, ordinary = portions_of(amount, rows * top, most, slope, True), portions_of(amount, rows * top, most, slope, False)
    places = jnp.arange(amount)

    def named(sizes, offset_by):
        used = int((sizes > 0).sum())
        fixed = max(1, used // 4)
        shifted = fixed + (places - fixed + offset_by * (used - fixed)) % max(1, amount - fixed)
        return jnp.zeros((amount,), jnp.int32).at[sequence[jnp.where(places < fixed, places, shifted)]].set(jnp.asarray(sizes, jnp.int32))

    sizes = jnp.where(number % 4 == 0, named(packed, number // 4), named(ordinary, number - number // 4 - 1))
    mixed = jax.random.permutation(jax.random.fold_in(own, 3), amount)
    donor, receiver = mixed[0:amount // 2 * 2:2], mixed[1:amount // 2 * 2:2]
    slack = jnp.minimum(sizes[donor] - 1, most - sizes[receiver]) // 2
    slack = jnp.where((donor == sequence[0]) | (receiver == sequence[0]) | (sizes[receiver] == 0), 0, jnp.maximum(slack, 0))
    shifted = jax.random.randint(jax.random.fold_in(own, 4), (amount // 2,), 0, 1 << 20) % (slack + 1)
    sizes = sizes.at[donor].add(-shifted).at[receiver].add(shifted)
    members = jnp.searchsorted(jnp.cumsum(sizes), jnp.arange(rows * top), side="right").astype(jnp.int32)
    table = members.reshape(top, rows).T
    table = table[jax.random.permutation(jax.random.fold_in(own, 1), rows)]
    offset_by = jax.random.randint(jax.random.fold_in(own, 2), (rows, 1), 0, top)
    return jnp.take_along_axis(table, (jnp.arange(top)[None, :] + offset_by) % top, axis=1)


def portions_of(amount, total, most, slope, full):
    loads = [(1 << 20) // math.isqrt(rank ** slope) + 1 for rank in range(1, amount + 1)]
    largest = most if full else min(most, max(-(-total // amount), total * loads[0] // sum(loads)))
    least = 1 if total - largest >= amount - 1 else 0
    given, surplus = [largest] + [least] * (amount - 1), total - largest - least * (amount - 1)
    while surplus > 0:
        free = [i for i in range(1, amount) if given[i] < largest] or [i for i in range(1, amount) if given[i] < most]
        pool, remaining = sum([loads[i] for i in free]), surplus
        for i in free:
            extra = min(most - given[i], max(1, remaining * loads[i] // pool), surplus)
            given[i] = given[i] + extra
            surplus = surplus - extra
    return np.array(given)


def noise(rng, shape, deviation, reach, pieces=(), kind=jnp.bfloat16):
    level = shard_levels(rng, shape, pieces, -0.22, 0.18) if pieces else 1.0
    entries = jax.random.normal(rng, shape, jnp.float32) * deviation * level
    return jnp.minimum(jnp.maximum(entries, -reach), reach).astype(kind)


def setup_inputs(seed: int = 0) -> dict:
    arg_keys = jax.random.split(jax.random.key(seed), 22)
    tokens = noise(arg_keys[0], (SEQS, D), 1.0, 6.0, ((0, 16),))
    cache_keys = noise(arg_keys[1], (SEQS, KVH, HD, CACHE), 1.0, 6.0, ((0, 16), (1, 2)))
    cache_values = noise(arg_keys[2], (SEQS, KVH, HD, CACHE), 1.0, 6.0, ((0, 16), (1, 2)))
    cache_lengths = draw_cache_lengths(jax.random.fold_in(arg_keys[21], 71), 0)
    norm_in = jnp.clip(1.0 + 0.18 * jax.random.normal(arg_keys[4], (D,), jnp.float32), 0.1, 1.9)
    w_query = noise(arg_keys[5], (D, HEADS * HD), D ** -0.5, 0.125, ((1, 2),))
    w_key = noise(arg_keys[6], (D, KVH * HD), D ** -0.5, 0.125, ((1, 2),))
    w_value = noise(arg_keys[7], (D, KVH * HD), D ** -0.5, 0.125, ((1, 2),))
    stick_bias = draw_stick_bias(jax.random.fold_in(arg_keys[21], 71), 0)
    w_output = noise(arg_keys[9], (HEADS * HD, D), HD ** -0.5, 0.75, ((0, 2),))
    norm_mid = jnp.clip(1.0 + 0.18 * jax.random.normal(arg_keys[10], (D,), jnp.float32), 0.1, 1.9)
    routes_keys = jax.random.split(jax.random.fold_in(arg_keys[11], 1), SEQS // SEQ_DEV)
    routes_turns = jax.random.permutation(jax.random.fold_in(arg_keys[11], 3), SEQS // SEQ_DEV)
    routes = jax.vmap(lambda own, number: deal_out(jax.random.fold_in(arg_keys[11], 2), own, number, SEQ_DEV, EXPERTS, TOPK, CAP, 1))(routes_keys, routes_turns).reshape((SEQS, TOPK))
    route_weights = jnp.clip(jnp.exp(math.log(1.0) - 2.3025851 * jax.random.uniform(arg_keys[12], (SEQS, TOPK), jnp.float32) ** shard_levels(arg_keys[12], (SEQS, TOPK), ((0, 16),), -0.2, 0.2)), 0.1, 1.0)
    expert_gate = noise(arg_keys[13], (EXPERTS, D, EW), D ** -0.5, 0.125, ((0, 16), (2, 2)))
    expert_up = noise(arg_keys[14], (EXPERTS, D, EW), D ** -0.5, 0.125, ((0, 16), (2, 2)))
    expert_down = noise(arg_keys[15], (EXPERTS, EW, D), EW ** -0.5, 0.25, ((0, 16), (1, 2)))
    dense_gate = noise(arg_keys[16], (D, SHARED), D ** -0.5, 0.125, ((0, 16),))
    dense_up = noise(arg_keys[17], (D, SHARED), D ** -0.5, 0.125, ((0, 16),))
    dense_down = noise(arg_keys[18], (SHARED, D), SHARED ** -0.5, 0.375, ((1, 16),))
    mix_gate = noise(arg_keys[19], (D,), D ** -0.5, 0.125, (), jnp.float32)
    norm_out = jnp.clip(1.0 + 0.18 * jax.random.normal(arg_keys[20], (D,), jnp.float32), 0.1, 1.9)
    return dict(tokens=tokens, cache_keys=cache_keys, cache_values=cache_values, cache_lengths=cache_lengths, norm_in=norm_in, w_query=w_query, w_key=w_key, w_value=w_value, stick_bias=stick_bias, w_output=w_output, norm_mid=norm_mid, routes=routes, route_weights=route_weights, expert_gate=expert_gate, expert_up=expert_up, expert_down=expert_down, dense_gate=dense_gate, dense_up=dense_up, dense_down=dense_down, mix_gate=mix_gate, norm_out=norm_out)


def layer_norm(values, gain):
    floats = values.astype(jnp.float32)
    center = lax.optimization_barrier(jnp.mean(floats, -1, keepdims=True))
    spread = lax.optimization_barrier(jnp.mean(jnp.square(floats - center), -1, keepdims=True))
    return (floats - center) * lax.rsqrt(spread + 1e-05) * gain

def rounded(values):
    return lax.optimization_barrier(values.astype(jnp.bfloat16)).astype(jnp.float32)

def reference(tokens, cache_keys, cache_values, cache_lengths, norm_in, w_query, w_key, w_value, stick_bias, w_output, norm_mid, routes, route_weights, expert_gate, expert_up, expert_down, dense_gate, dense_up, dense_down, mix_gate, norm_out):
    normed = layer_norm(tokens, norm_in).astype(jnp.bfloat16)
    queries = jnp.dot(normed, w_query, preferred_element_type=jnp.float32).astype(jnp.bfloat16)
    fresh_keys = jnp.dot(normed, w_key, preferred_element_type=jnp.float32).astype(jnp.bfloat16)
    fresh_values = jnp.dot(normed, w_value, preferred_element_type=jnp.float32).astype(jnp.bfloat16)
    groups = HEADS // KVH
    bias_grid = stick_bias.astype(jnp.float32).reshape(KVH, groups)

    def attend(inputs):
        query_block, key_block, value_block, length_block = inputs
        query_grid = query_block.reshape(SEQ_DEV, KVH, groups, HD).astype(jnp.float32)
        scores = jnp.einsum('bkgd,bkdc->bkgc', query_grid, key_block.astype(jnp.float32)) * HD ** (-0.5)
        scores = scores + bias_grid[None, :, :, None]
        visible = (jnp.arange(CACHE)[None, :] < length_block[:, None])[:, None, None, :]
        log_keep = jnp.where(visible, jax.nn.log_sigmoid(-scores), 0.0)
        later_sum = lax.cumsum(log_keep, axis=3, reverse=True) - log_keep
        stick = jnp.where(visible, jnp.exp(jax.nn.log_sigmoid(scores) + later_sum), 0.0).astype(jnp.bfloat16)
        output = jnp.einsum('bkgc,bkdc->bkgd', stick.astype(jnp.float32), value_block.astype(jnp.float32))
        return output.reshape(SEQ_DEV, HEADS * HD).astype(jnp.bfloat16)
    block_count = SEQS // SEQ_DEV
    attended = lax.map(attend, (queries.reshape(block_count, SEQ_DEV, HEADS * HD), cache_keys.reshape(block_count, SEQ_DEV, KVH, HD, CACHE), cache_values.reshape(block_count, SEQ_DEV, KVH, HD, CACHE), cache_lengths.reshape(block_count, SEQ_DEV)))
    attended = attended.reshape(SEQS, HEADS * HD)
    projected = jnp.dot(attended, w_output, preferred_element_type=jnp.float32)
    hidden = layer_norm(normed.astype(jnp.float32) + projected, norm_mid).astype(jnp.bfloat16)
    slots = N_EP * CAP
    part_width = EW // N_TP

    def run_expert(inputs):
        number, gate_w, up_w, down_w = inputs
        is_hit = routes == number
        weight_sum = lax.optimization_barrier(jnp.sum(jnp.where(is_hit, route_weights, 0.0), axis=1))
        is_used = jnp.any(is_hit, axis=1)
        picked = jnp.nonzero(is_used, size=slots, fill_value=0)[0].astype(jnp.int32)
        is_valid = (jnp.arange(slots) < jnp.sum(is_used.astype(jnp.int32))).astype(weight_sum.dtype)
        token_rows = hidden[picked]
        gate_pre = jnp.dot(token_rows, gate_w, preferred_element_type=jnp.float32)
        up_pre = jnp.dot(token_rows, up_w, preferred_element_type=jnp.float32)
        act = (jax.nn.silu(gate_pre) * up_pre).astype(jnp.bfloat16)
        combined = jnp.zeros((slots, D), gate_pre.dtype)
        for index in range(N_TP):
            partial_value = jnp.dot(act[:, index * part_width:(index + 1) * part_width], down_w[index * part_width:(index + 1) * part_width], preferred_element_type=jnp.float32)
            combined = combined + rounded(partial_value)
        expert_out = rounded(combined)
        return (picked, expert_out * (weight_sum[picked] * is_valid)[:, None])
    picked_all, terms = lax.map(run_expert, (jnp.arange(EXPERTS).astype(jnp.int32), expert_gate, expert_up, expert_down))
    routed = jax.ops.segment_sum(terms.reshape(-1, D), picked_all.reshape(-1), num_segments=SEQS)
    dense_pre = jnp.dot(hidden, dense_gate, preferred_element_type=jnp.float32)
    dense_lin = jnp.dot(hidden, dense_up, preferred_element_type=jnp.float32)
    dense_act = (jax.nn.silu(dense_pre) * dense_lin).astype(jnp.bfloat16)
    dense_out = jnp.dot(dense_act, dense_down, preferred_element_type=jnp.float32)
    mix_weight = jax.nn.sigmoid(jnp.dot(hidden.astype(jnp.float32), mix_gate, precision=lax.Precision.HIGHEST))
    combined_rows = hidden.astype(jnp.float32) + routed + mix_weight[:, None] * dense_out
    mixed = layer_norm(combined_rows, norm_out).astype(jnp.bfloat16)
    return (mixed, fresh_keys, fresh_values)
```

```python
import jax
import jax.numpy as jnp
from jax import lax
from jax.sharding import PartitionSpec as P


def layer_norm(values, gain):
    floats = values.astype(jnp.float32)
    center = jnp.mean(floats, -1, keepdims=True)
    spread = jnp.mean(jnp.square(floats - center), -1, keepdims=True)
    return (floats - center) * lax.rsqrt(spread + 1e-05) * gain


def later_positions(log_keep):
    length = log_keep.shape[-1]
    span = 128
    count = length // span
    lead = log_keep.shape[:-1]
    blocks = log_keep.reshape(lead + (count, span))
    inner = jnp.arange(span)
    within_table = (inner[:, None] > inner[None, :]).astype(jnp.float32)
    within = jnp.einsum("...nb,bc->...nc", blocks, within_table, precision=lax.Precision.HIGHEST)
    totals = jnp.sum(blocks, axis=-1)
    outer = jnp.arange(count)
    outer_table = (outer[:, None] > outer[None, :]).astype(jnp.float32)
    carried = jnp.einsum("...m,mn->...n", totals, outer_table, precision=lax.Precision.HIGHEST)
    return (within + carried[..., None]).reshape(lead + (length,))


def swap_core(values):
    return lax.ppermute(values, "tp", [(0, 1), (1, 0)])


def join_halves(own, other, core):
    low = jnp.where(core == 0, own, other)
    high = jnp.where(core == 0, other, own)
    return jnp.concatenate([low, high], axis=-1)


def shards(
    tokens,
    cache_keys,
    cache_values,
    cache_lengths,
    norm_in,
    w_query,
    w_key,
    w_value,
    stick_bias,
    w_output,
    norm_mid,
    routes,
    route_weights,
    expert_gate,
    expert_up,
    expert_down,
    dense_gate,
    dense_up,
    dense_down,
    mix_gate,
    norm_out,
):
    share = dense_gate.shape[1] // lax.axis_size("tp")
    rows = dense_gate.shape[0]
    ep_count = lax.axis_size("ep")
    offset = lax.axis_index("tp") * share
    gate_share = lax.dynamic_slice_in_dim(dense_gate, offset, share, 1)
    up_share = lax.dynamic_slice_in_dim(dense_up, offset, share, 1)
    down_share = lax.dynamic_slice_in_dim(dense_down, offset, share, 0)
    packed = jnp.concatenate(
        [gate_share.reshape(-1), up_share.reshape(-1), down_share.reshape(-1)]
    ).reshape(1, -1, 128)
    packed = jnp.broadcast_to(packed, (ep_count,) + packed.shape[1:])
    gathered = lax.all_to_all(packed, "ep", split_axis=0, concat_axis=0, tiled=True)
    gathered = gathered.reshape(ep_count, 3, rows * share)
    gate_full = gathered[:, 0].reshape(ep_count * rows, share)
    up_full = gathered[:, 1].reshape(ep_count * rows, share)
    down_full = jnp.moveaxis(gathered[:, 2].reshape(ep_count, share, -1), 0, 1).reshape(share, -1)
    normed = layer_norm(tokens, norm_in).astype(jnp.bfloat16)
    queries = jnp.dot(normed, w_query, preferred_element_type=jnp.float32).astype(jnp.bfloat16)
    fresh_keys = jnp.dot(normed, w_key, preferred_element_type=jnp.float32).astype(jnp.bfloat16)
    fresh_values = jnp.dot(normed, w_value, preferred_element_type=jnp.float32).astype(jnp.bfloat16)
    sequences = tokens.shape[0]
    kv_local = cache_keys.shape[1]
    head_dim = cache_keys.shape[2]
    length = cache_keys.shape[3]
    heads_local = stick_bias.shape[0]
    groups = heads_local // kv_local
    query_grid = queries.reshape(sequences, kv_local, groups, head_dim)
    scores = jnp.einsum(
        "skgd,skdc->skgc", query_grid, cache_keys, preferred_element_type=jnp.float32
    ) * head_dim ** (-0.5)
    scores = scores + stick_bias.reshape(kv_local, groups)[None, :, :, None]
    visible = (jnp.arange(length)[None, :] < cache_lengths[:, None])[:, None, None, :]
    log_keep = jnp.where(visible, jax.nn.log_sigmoid(-scores), 0.0)
    later_sum = later_positions(log_keep)
    stick = jnp.where(visible, jnp.exp(jax.nn.log_sigmoid(scores) + later_sum), 0.0).astype(
        jnp.bfloat16
    )
    attended = jnp.einsum(
        "skgc,skdc->skgd", stick, cache_values, preferred_element_type=jnp.float32
    )
    attended = attended.reshape(sequences, heads_local * head_dim).astype(jnp.bfloat16)
    partial_proj = jnp.dot(attended, w_output, preferred_element_type=jnp.float32)
    projected = partial_proj + swap_core(partial_proj)
    hidden = layer_norm(normed.astype(jnp.float32) + projected, norm_mid).astype(jnp.bfloat16)
    width = hidden.shape[1]
    topk = routes.shape[1]
    experts = ep_count * expert_gate.shape[0]
    capacity = max(2, (sequences * topk + ep_count - 1) // ep_count)
    flat_routes = routes.reshape(-1)
    onehot = (flat_routes[:, None] == jnp.arange(experts)[None, :]).astype(jnp.float32)
    flat_count = flat_routes.shape[0]
    row_index = jnp.arange(flat_count)
    earlier_table = (row_index[:, None] > row_index[None, :]).astype(jnp.float32)
    before = jnp.dot(earlier_table, onehot, precision=lax.Precision.HIGHEST)
    slot_index = jnp.sum(before * onehot, axis=1).astype(jnp.int32)
    target = flat_routes * capacity + slot_index
    placement = jnp.arange(experts * capacity)[:, None] == target[None, :]
    dispatch = jnp.any(placement.reshape(experts * capacity, sequences, topk), axis=2).astype(
        jnp.bfloat16
    )
    outgoing = jnp.dot(dispatch, hidden, preferred_element_type=jnp.float32).astype(jnp.bfloat16)
    half = width // lax.axis_size("tp")
    core = lax.axis_index("tp")
    mine = lax.dynamic_slice_in_dim(outgoing, core * half, half, 1)
    received = lax.all_to_all(
        mine.reshape(ep_count, capacity, half), "ep", split_axis=0, concat_axis=0, tiled=True
    ).reshape(-1, half)
    token_rows = join_halves(received, swap_core(received), core)
    gate_pre = jnp.dot(token_rows, expert_gate[0], preferred_element_type=jnp.float32)
    up_pre = jnp.dot(token_rows, expert_up[0], preferred_element_type=jnp.float32)
    act = (jax.nn.silu(gate_pre) * up_pre).astype(jnp.bfloat16)
    partial_out = jnp.dot(act, expert_down[0], preferred_element_type=jnp.float32).astype(
        jnp.bfloat16
    )
    kept = lax.dynamic_slice_in_dim(partial_out, core * half, half, 1)
    sent = lax.dynamic_slice_in_dim(partial_out, (1 - core) * half, half, 1)
    expert_out = (kept.astype(jnp.float32) + swap_core(sent).astype(jnp.float32)).astype(
        jnp.bfloat16
    )
    returned = lax.all_to_all(
        expert_out.reshape(ep_count, capacity, half), "ep", split_axis=0, concat_axis=0, tiled=True
    ).reshape(-1, half)
    selector = jnp.transpose(placement).astype(jnp.bfloat16)
    picked = jnp.dot(selector, returned, preferred_element_type=jnp.float32)
    routed = jnp.sum(picked.reshape(sequences, topk, half) * route_weights[:, :, None], axis=1)
    routed = join_halves(routed, swap_core(routed), core)
    dense_pre = jnp.dot(hidden, gate_full, preferred_element_type=jnp.float32)
    dense_lin = jnp.dot(hidden, up_full, preferred_element_type=jnp.float32)
    dense_act = (jax.nn.silu(dense_pre) * dense_lin).astype(jnp.bfloat16)
    dense_part = jnp.dot(dense_act, down_full, preferred_element_type=jnp.float32)
    dense_out = dense_part + swap_core(dense_part)
    mix_weight = jax.nn.sigmoid(
        jnp.dot(hidden.astype(jnp.float32), mix_gate, precision=lax.Precision.HIGHEST)
    )
    combined_rows = hidden.astype(jnp.float32) + routed + mix_weight[:, None] * dense_out
    mixed_rows = layer_norm(combined_rows, norm_out).astype(jnp.bfloat16)
    return (mixed_rows, fresh_keys, fresh_values)


def solution(mesh):
    in_specs = (
        P("ep", None),
        P("ep", "tp", None, None),
        P("ep", "tp", None, None),
        P("ep"),
        P(),
        P(None, "tp"),
        P(None, "tp"),
        P(None, "tp"),
        P("tp"),
        P("tp", None),
        P(),
        P("ep", None),
        P("ep", None),
        P("ep", None, "tp"),
        P("ep", None, "tp"),
        P("ep", "tp", None),
        P("ep", None),
        P("ep", None),
        P(None, "ep"),
        P(),
        P(),
    )
    out_specs = (P("ep", None), P("ep", "tp"), P("ep", "tp"))
    return jax.shard_map(shards, mesh=mesh, in_specs=in_specs, out_specs=out_specs, check_vma=False)
```

```python
import functools

import jax
import jax.numpy as jnp
from jax import lax
from jax.experimental import pallas as pl
from jax.experimental.pallas import tpu as pltpu
from jax.sharding import PartitionSpec as P

LANES = 128
F32 = jnp.float32
BF16 = jnp.bfloat16
VMEM = pltpu.VMEM
SMEM = pltpu.SMEM
HBM = pltpu.MemorySpace.HBM


def in_vmem():
    return pl.BlockSpec(memory_space=VMEM)


def in_smem():
    return pl.BlockSpec(memory_space=SMEM)


def in_hbm():
    return pl.BlockSpec(memory_space=HBM)


def params(mib):
    return pltpu.CompilerParams(vmem_limit_bytes=mib << 20)


def cost(flops, moved):
    return pl.CostEstimate(flops=flops, bytes_accessed=moved, transcendentals=0)


def iota(shape, dim):
    return lax.broadcasted_iota(jnp.int32, shape, dim)


def dot(a, b):
    return jnp.dot(a, b, preferred_element_type=F32)


def dot_last(a, b):
    return lax.dot_general(a, b, (((1,), (1,)), ((), ())), preferred_element_type=F32)


def dot_first(a, b):
    return lax.dot_general(a, b, (((0,), (0,)), ((), ())), preferred_element_type=F32)


def norm_rows(floats, gain):
    center = jnp.mean(floats, -1, keepdims=True)
    shifted = floats - center
    spread = jnp.mean(jnp.square(shifted), -1, keepdims=True)
    return shifted * lax.rsqrt(spread + 1e-05) * gain


def split_high(values):
    high = values.astype(BF16)
    return high, values - high.astype(F32)


def attention_kernel(
    lengths, bias, tokens, gain, wq_hbm, k_hbm, v_hbm, wo_hbm, partial, normed, wq, k, v, wo, sems
):
    copies = [
        pltpu.make_async_copy(src, dst, sems.at[i])
        for i, (src, dst) in enumerate(((wq_hbm, wq), (k_hbm, k), (v_hbm, v), (wo_hbm, wo)))
    ]
    for copy in copies:
        copy.start()
    sequences = tokens.shape[0]
    heads = wq.shape[1] * 2 // LANES
    head_dim = LANES // 2
    length = k.shape[1]
    rows = heads * sequences
    wide = sequences * head_dim
    rounded = norm_rows(tokens[...].astype(F32), gain[...]).astype(BF16)
    normed[...] = rounded
    copies[0].wait()
    queries = dot(rounded, wq[...]).astype(BF16).astype(F32) * head_dim ** (-0.5)
    low_lane = iota((sequences, LANES), 1) < head_dim
    own_block = iota((sequences, wide), 1) // head_dim == iota((sequences, wide), 0)
    blocks = []
    for h in range(heads):
        slab = queries[:, h // 2 * LANES : (h // 2 + 1) * LANES]
        turned = pltpu.roll(slab, head_dim, 1)
        both = jnp.where(low_lane, slab, turned) if h % 2 == 0 else jnp.where(low_lane, turned, slab)
        blocks.append(jnp.where(own_block, jnp.concatenate([both] * (wide // LANES), axis=1), 0.0))
    spread_queries = jnp.concatenate(blocks, axis=0).astype(BF16)

    row = iota((rows, 1), 0)
    limit = jnp.zeros((rows, 1), jnp.int32)
    for s in range(sequences):
        limit = jnp.where(row % sequences == s, lengths[s], limit)
    offset = jnp.zeros((rows, 1), F32)
    for h in range(heads):
        offset = jnp.where(row // sequences == h, bias[h], offset)
    visible = iota((rows, length), 1) < limit

    copies[1].wait()
    scores = dot(spread_queries, k[...]) + offset
    tail = jnp.log1p(jnp.exp(-jnp.abs(scores)))
    keep = jnp.where(visible, -(jnp.maximum(scores, 0.0) + tail), 0.0)
    high, rest = split_high(keep)
    middle, rest = split_high(rest)
    low = rest.astype(BF16)
    span = 2 * LANES
    count = length // span
    pieces = [part[:, n * span : (n + 1) * span] for part in (high, middle, low) for n in range(count)]
    after = (iota((span, span), 0) > iota((span, span), 1)).astype(BF16)
    sums = dot(jnp.concatenate(pieces, axis=0), after)
    carry = jnp.zeros((rows, 1), F32)
    later = [None] * count
    for n in reversed(range(count)):
        within = (
            sums[n * rows : (n + 1) * rows]
            + sums[(count + n) * rows : (count + n + 1) * rows]
            + sums[(2 * count + n) * rows : (2 * count + n + 1) * rows]
        )
        later[n] = within + carry
        carry = carry + within[:, 0:1] + keep[:, n * span : n * span + 1]
    later_sum = jnp.concatenate(later, axis=1)
    stick = jnp.where(visible, jnp.exp(jnp.minimum(scores, 0.0) - tail + later_sum), 0.0).astype(BF16)

    copies[2].wait()
    mixed = dot_last(stick, v[...])
    own_rows = iota((rows, wide), 1) // head_dim == iota((rows, wide), 0) % sequences
    mixed = jnp.where(own_rows, mixed, 0.0)
    folded = mixed[:, 0:LANES]
    for j in range(1, wide // LANES):
        folded = folded + mixed[:, j * LANES : (j + 1) * LANES]
    folded = folded + pltpu.roll(folded, head_dim, 1)
    slabs = [
        jnp.where(
            low_lane,
            folded[h * sequences : (h + 1) * sequences],
            folded[(h + 1) * sequences : (h + 2) * sequences],
        )
        for h in range(0, heads, 2)
    ]
    attended = jnp.concatenate(slabs, axis=1).astype(BF16)
    copies[3].wait()
    partial[...] = dot(attended, wo[...])


def attention(tokens, gain, w_query, keys, values, lengths, bias, w_output):
    sequences, kv_local, head_dim, length = keys.shape
    assert kv_local == 1 and head_dim * 2 == LANES
    width = tokens.shape[1]
    wide = sequences * head_dim
    flat = (wide, length)
    return pl.pallas_call(
        attention_kernel,
        out_shape=(
            jax.ShapeDtypeStruct((sequences, width), F32),
            jax.ShapeDtypeStruct((sequences, width), BF16),
        ),
        in_specs=[in_smem(), in_smem(), in_vmem(), in_vmem()] + [in_hbm()] * 4,
        out_specs=(in_vmem(), in_vmem()),
        scratch_shapes=[
            VMEM(w_query.shape, BF16),
            VMEM(flat, BF16),
            VMEM(flat, BF16),
            VMEM(w_output.shape, BF16),
            pltpu.SemaphoreType.DMA((4,)),
        ],
        compiler_params=params(58),
        cost_estimate=cost(1 << 32, 7 << 20),
        name="attention",
    )(lengths, bias, tokens, gain.reshape(1, -1), w_query, keys.reshape(flat), values.reshape(flat), w_output)


def plan_kernel(capacity, routes, weights, place, share):
    topk, sequences = routes.shape
    slots = place.shape[0]
    expert = iota((slots, sequences), 0) // capacity
    hit = jnp.zeros((slots, sequences), F32)
    weight = jnp.zeros((slots, sequences), F32)
    for j in range(topk):
        match = routes[j : j + 1, :] == expert
        hit = jnp.where(match, 1.0, hit)
        weight = jnp.where(match, weights[j : j + 1, :], weight)
    earlier = (iota((sequences, sequences), 0) < iota((sequences, sequences), 1)).astype(BF16)
    rank = dot(hit.astype(BF16), earlier)
    turn = (iota((slots, sequences), 0) % capacity).astype(F32)
    chosen = (hit > 0.0) & (rank == turn)
    place[...] = jnp.where(chosen, 1.0, 0.0).astype(BF16)
    share[...] = jnp.where(chosen, weight, 0.0)


def plan(routes, route_weights, slots, capacity):
    sequences = routes.shape[0]
    return pl.pallas_call(
        functools.partial(plan_kernel, capacity),
        out_shape=(
            jax.ShapeDtypeStruct((slots, sequences), BF16),
            jax.ShapeDtypeStruct((slots, sequences), F32),
        ),
        in_specs=[in_vmem(), in_vmem()],
        out_specs=(in_vmem(), in_vmem()),
        compiler_params=params(8),
        cost_estimate=cost(1 << 20, 1 << 16),
        name="plan",
    )(jnp.transpose(routes), jnp.transpose(route_weights))


def store_rows(scratch, values):
    count, width = values.shape
    parts = width // LANES
    for j in range(parts):
        scratch[pl.ds(j, count, stride=parts), :] = values[:, j * LANES : (j + 1) * LANES]


def load_rows(scratch, count):
    parts = scratch.shape[0] // count
    return jnp.concatenate(
        [scratch[pl.ds(j, count, stride=parts), :] for j in range(parts)], axis=1
    )


def half_of(ref, core, half):
    return ref[:, pl.ds(pl.multiple_of(core * half, half), half)]


def middle_kernel(partial, other, normed, gain, place, hidden, outgoing, scratch):
    _, width = partial.shape
    half = width // 2
    floats = normed[...].astype(F32) + (partial[...] + other[...])
    hidden[...] = norm_rows(floats, gain[...]).astype(BF16)
    mine = half_of(hidden, lax.axis_index("tp"), half)
    store_rows(scratch, dot(place[...], mine))
    outgoing[...] = scratch[...].astype(BF16)


def middle(partial, other, normed, gain, place):
    sequences, width = partial.shape
    packed = (place.shape[0] * (width // 2) // LANES, LANES)
    return pl.pallas_call(
        middle_kernel,
        out_shape=(
            jax.ShapeDtypeStruct((sequences, width), BF16),
            jax.ShapeDtypeStruct(packed, BF16),
        ),
        in_specs=[in_vmem()] * 5,
        out_specs=(in_vmem(), in_vmem()),
        scratch_shapes=[VMEM(packed, F32)],
        compiler_params=params(12),
        cost_estimate=cost(1 << 28, 1 << 20),
        name="middle",
    )(partial, other, normed, gain.reshape(1, -1), place)


def expert_kernel(own, other, gate, up, down, kept, sent, scratch, rows):
    core = lax.axis_index("tp")
    packed = own.shape[0]
    width = gate.shape[0]
    half = width // 2
    count = packed * LANES // half
    scratch[...] = own[...].astype(F32)
    own_rows = load_rows(scratch, count).astype(BF16)
    scratch[...] = other[...].astype(F32)
    other_rows = load_rows(scratch, count).astype(BF16)
    rows[:, pl.ds(pl.multiple_of(core * half, half), half)] = own_rows
    rows[:, pl.ds(pl.multiple_of((1 - core) * half, half), half)] = other_rows
    inputs = rows[...]
    gate_pre = dot(inputs, gate[...])
    up_pre = dot(inputs, up[...])
    act = (jax.nn.silu(gate_pre) * up_pre).astype(BF16)
    store_rows(scratch, dot(act, half_of(down, core, half)))
    kept[...] = scratch[...].astype(BF16)
    store_rows(scratch, dot(act, half_of(down, 1 - core, half)))
    sent[...] = scratch[...].astype(BF16)


def expert(own, other, gate, up, down):
    packed = own.shape
    width = gate.shape[0]
    count = packed[0] * LANES * 2 // width
    return pl.pallas_call(
        expert_kernel,
        out_shape=(jax.ShapeDtypeStruct(packed, BF16), jax.ShapeDtypeStruct(packed, BF16)),
        in_specs=[in_vmem()] * 5,
        out_specs=(in_vmem(), in_vmem()),
        scratch_shapes=[VMEM(packed, F32), VMEM((count, width), BF16)],
        compiler_params=params(24),
        cost_estimate=cost(1 << 30, 4 << 20),
        name="expert",
    )(own, other, gate, up, down)


def add_kernel(a, b, out):
    out[...] = (a[...].astype(F32) + b[...].astype(F32)).astype(BF16)


def add_rounded(a, b):
    return pl.pallas_call(
        add_kernel,
        out_shape=jax.ShapeDtypeStruct(a.shape, BF16),
        in_specs=[in_vmem()] * 2,
        out_specs=in_vmem(),
        compiler_params=params(4),
        cost_estimate=cost(1 << 18, 1 << 19),
        name="add_parts",
    )(a, b)


def combine_kernel(returned, share, out, scratch):
    scratch[...] = returned[...].astype(F32)
    rows = load_rows(scratch, share.shape[0]).astype(BF16)
    high, rest = split_high(share[...])
    out[...] = dot_first(high, rows) + dot_first(rest.astype(BF16), rows)


def combine(returned, share):
    half = returned.shape[0] * LANES // share.shape[0]
    return pl.pallas_call(
        combine_kernel,
        out_shape=jax.ShapeDtypeStruct((share.shape[1], half), F32),
        in_specs=[in_vmem()] * 2,
        out_specs=in_vmem(),
        scratch_shapes=[VMEM(returned.shape, F32)],
        compiler_params=params(8),
        cost_estimate=cost(1 << 24, 1 << 19),
        name="combine",
    )(returned, share)


def last_kernel(own, other, dense, dense_other, hidden, mix_gate, gain, mixed, total):
    core = lax.axis_index("tp")
    half = own.shape[1]
    floats = hidden[...].astype(F32)
    mix = jax.nn.sigmoid(jnp.sum(floats * mix_gate[...], axis=-1, keepdims=True))
    total[...] = floats + mix * (dense[...] + dense_other[...])
    mine = pl.ds(pl.multiple_of(core * half, half), half)
    theirs = pl.ds(pl.multiple_of((1 - core) * half, half), half)
    total[:, mine] = total[:, mine] + own[...]
    total[:, theirs] = total[:, theirs] + other[...]
    mixed[...] = norm_rows(total[...], gain[...]).astype(BF16)


def last(own, other, dense, dense_other, hidden, mix_gate, gain):
    return pl.pallas_call(
        last_kernel,
        out_shape=jax.ShapeDtypeStruct(hidden.shape, BF16),
        in_specs=[in_vmem()] * 7,
        out_specs=in_vmem(),
        scratch_shapes=[VMEM(hidden.shape, F32)],
        compiler_params=params(8),
        cost_estimate=cost(1 << 20, 1 << 20),
        name="last",
    )(own, other, dense, dense_other, hidden, mix_gate.reshape(1, -1), gain.reshape(1, -1))


def fresh_kernel(normed, w_key, w_value, keys, values):
    rows = normed[...]
    keys[...] = dot_last(rows, w_key[...]).astype(BF16)
    values[...] = dot_last(rows, w_value[...]).astype(BF16)


def fresh(normed, w_key, w_value):
    shape = jax.ShapeDtypeStruct((normed.shape[0], w_key.shape[1]), BF16)
    return pl.pallas_call(
        fresh_kernel,
        out_shape=(shape, shape),
        in_specs=[in_vmem()] * 3,
        out_specs=(in_vmem(), in_vmem()),
        compiler_params=params(8),
        cost_estimate=cost(1 << 24, 1 << 19),
        name="fresh",
    )(normed, jnp.transpose(w_key), jnp.transpose(w_value))


def swap_core(values):
    return lax.ppermute(values, "tp", [(0, 1), (1, 0)])


def exchange(packed, ep_count):
    blocks = packed.reshape(ep_count, -1, LANES)
    moved = lax.all_to_all(blocks, "ep", split_axis=0, concat_axis=0, tiled=True)
    return moved.reshape(packed.shape)


def swap_far(values, bit):
    count = lax.axis_size("ep")
    return lax.ppermute(values, "ep", [(i, i ^ bit) for i in range(count)])


def pack_kernel(gate, up, down, packed):
    core = lax.axis_index("tp")
    rows, units = gate.shape
    share = units // 2
    packed[0:rows, 0:share] = half_of(gate, core, share)
    packed[0:rows, share:units] = half_of(up, core, share)
    mine = down[pl.ds(pl.multiple_of(core * share, share), share), :]
    packed[rows:, 0:share] = mine[0 : share // 2]
    packed[rows:, share:units] = mine[share // 2 : share]


def pack(gate, up, down):
    rows, units = gate.shape
    return pl.pallas_call(
        pack_kernel,
        out_shape=jax.ShapeDtypeStruct((rows + units // 4, units), BF16),
        in_specs=[in_vmem()] * 3,
        out_specs=in_vmem(),
        compiler_params=params(8),
        cost_estimate=cost(1 << 18, 1 << 18),
        name="pack",
    )(gate, up, down)


def join_kernel(*refs):
    out, at = refs[-1], 0
    for ref in refs[:-1]:
        out[at : at + ref.shape[0], :] = ref[...]
        at += ref.shape[0]


def join(*blocks):
    rows = sum(block.shape[0] for block in blocks)
    return pl.pallas_call(
        join_kernel,
        out_shape=jax.ShapeDtypeStruct((rows, blocks[0].shape[1]), BF16),
        in_specs=[in_vmem()] * len(blocks),
        out_specs=in_vmem(),
        compiler_params=params(8),
        cost_estimate=cost(1 << 18, 1 << 19),
        name="join",
    )(*blocks)


def dense_kernel(offsets, hidden, *refs):
    sources, out = refs[:-1], refs[-1]
    units = sources[0].shape[1]
    share = units // 2
    rows = LANES
    height = rows + share // 2
    me = lax.axis_index("ep")
    blocks = []
    for ref, group in zip(sources, offsets):
        for n, offset in enumerate(group):
            blocks.append((ref, n * height, (me ^ offset) * rows))
    pre = jnp.zeros((hidden.shape[0], units), F32)
    for j in range(0, len(blocks), 2):
        left = [hidden[:, pl.ds(pl.multiple_of(at, rows), rows)] for _, _, at in blocks[j : j + 2]]
        right = [ref[start : start + rows, :] for ref, start, _ in blocks[j : j + 2]]
        pre = pre + dot(jnp.concatenate(left, axis=1), jnp.concatenate(right, axis=0))
    act = (jax.nn.silu(pre[:, 0:share]) * pre[:, share:units]).astype(BF16)
    for ref, start, at in blocks:
        tail = ref[start + rows : start + height, :]
        down = jnp.concatenate([tail[:, 0:share], tail[:, share:units]], axis=0)
        out[:, pl.ds(pl.multiple_of(at, rows), rows)] = dot(act, down)


def dense(hidden, sources, offsets):
    return pl.pallas_call(
        functools.partial(dense_kernel, offsets),
        out_shape=jax.ShapeDtypeStruct(hidden.shape, F32),
        in_specs=[in_vmem()] * (1 + len(sources)),
        out_specs=in_vmem(),
        compiler_params=params(8),
        cost_estimate=cost(1 << 28, 2 << 20),
        name="dense",
    )(hidden, *sources)


def dense_weights(dense_gate, dense_up, dense_down):
    share = dense_gate.shape[1] // lax.axis_size("tp")
    offset = lax.axis_index("tp") * share
    gate = lax.dynamic_slice_in_dim(dense_gate, offset, share, 1)
    up = lax.dynamic_slice_in_dim(dense_up, offset, share, 1)
    down = lax.dynamic_slice_in_dim(dense_down, offset, share, 0)
    return jnp.concatenate(
        [gate.reshape(-1, LANES), up.reshape(-1, LANES), down.reshape(-1, LANES)]
    )


def dense_narrow(hidden, packed, rows, share):
    count = lax.axis_size("ep")
    packed = packed[None]
    bits = [count >> (n + 1) for n in range(count.bit_length() - 1)]
    for bit in bits:
        packed = jnp.concatenate([packed, swap_far(packed, bit)])
    order = [0] * count
    for j in range(count):
        order[sum(bit for n, bit in enumerate(bits) if j >> n & 1)] = j
    packed = jnp.take(packed[jnp.array(order)], lax.axis_index("ep") ^ jnp.arange(count), axis=0)
    packed = packed.reshape(count, 3, rows * share)
    gate = packed[:, 0].reshape(count * rows, share)
    up = packed[:, 1].reshape(count * rows, share)
    down = jnp.moveaxis(packed[:, 2].reshape(count, share, rows), 0, 1).reshape(share, -1)
    act = (jax.nn.silu(dot(hidden, gate)) * dot(hidden, up)).astype(BF16)
    return dot(act, down)


def shards(
    tokens,
    cache_keys,
    cache_values,
    cache_lengths,
    norm_in,
    w_query,
    w_key,
    w_value,
    stick_bias,
    w_output,
    norm_mid,
    routes,
    route_weights,
    expert_gate,
    expert_up,
    expert_down,
    dense_gate,
    dense_up,
    dense_down,
    mix_gate,
    norm_out,
):
    sequences, topk = routes.shape
    ep_count = lax.axis_size("ep")
    experts = ep_count * expert_gate.shape[0]
    capacity = max(2, (sequences * topk + ep_count - 1) // ep_count)
    slots = experts * capacity
    rows = dense_gate.shape[0]
    share = dense_gate.shape[1] // lax.axis_size("tp")
    wide = rows == LANES and share == LANES
    if wide:
        block = pack(dense_gate, dense_up, dense_down)
        columns = [0]
        bit = ep_count // 2
        far = []
        while bit > 2:
            far.append(swap_far(block, bit))
            columns = columns + [c ^ bit for c in columns]
            if bit > 4 or bit == 4:
                block = join(block, far[-1])
            bit //= 2
    partial, normed = attention(
        tokens, norm_in, w_query, cache_keys, cache_values, cache_lengths, stick_bias, w_output
    )
    place, portion = plan(routes, route_weights, slots, capacity)
    partial_other = swap_core(partial)
    hidden, outgoing = middle(partial, partial_other, normed, norm_mid, place)
    received = exchange(outgoing, ep_count)
    received_other = swap_core(received)
    kept, sent = expert(received, received_other, expert_gate[0], expert_up[0], expert_down[0])
    sent_other = swap_core(sent)
    summed = add_rounded(kept, sent_other)
    returned = exchange(summed, ep_count)
    fresh_keys, fresh_values = fresh(normed, w_key, w_value)
    if wide:
        from_x = swap_far(block, 1)
        from_y = swap_far(block, 2)
        part = block.shape[0] // 2
        diagonal_low = swap_far(from_y[:part], 1)
        diagonal_high = swap_far(from_x[part:], 2)
        count = len(columns) // 2
        offsets = (
            tuple(columns),
            tuple(c ^ 1 for c in columns),
            tuple(c ^ 2 for c in columns),
            tuple(c ^ 3 for c in columns[:count]),
            tuple(c ^ 3 for c in columns[count:]),
        )
        dense_out = dense(hidden, (block, from_x, from_y, diagonal_low, diagonal_high), offsets)
    else:
        packed = dense_weights(dense_gate, dense_up, dense_down)
        dense_out = dense_narrow(hidden, packed, rows, share)
    dense_other = swap_core(dense_out)
    own = combine(returned, portion)
    own_other = swap_core(own)
    mixed = last(own, own_other, dense_out, dense_other, hidden, mix_gate, norm_out)
    return (mixed, fresh_keys, fresh_values)


def solution(mesh):
    in_specs = (
        P("ep", None),
        P("ep", "tp", None, None),
        P("ep", "tp", None, None),
        P("ep"),
        P(),
        P(None, "tp"),
        P(None, "tp"),
        P(None, "tp"),
        P("tp"),
        P("tp", None),
        P(),
        P("ep", None),
        P("ep", None),
        P("ep", None, "tp"),
        P("ep", None, "tp"),
        P("ep", "tp", None),
        P("ep", None),
        P("ep", None),
        P(None, "ep"),
        P(),
        P(),
    )
    out_specs = (P("ep", None), P("ep", "tp"), P("ep", "tp"))
    return jax.shard_map(shards, mesh=mesh, in_specs=in_specs, out_specs=out_specs, check_vma=False)
```

```python
import functools

import jax
import jax.numpy as jnp
from jax import lax
from jax.experimental import pallas as pl
from jax.experimental.pallas import tpu as pltpu
from jax.sharding import PartitionSpec as P


LANES = 128
CHUNKS = 4
F32 = jnp.float32
BF16 = jnp.bfloat16
VMEM = pltpu.VMEM
SMEM = pltpu.SMEM
HBM = pltpu.MemorySpace.HBM


def in_vmem():
    return pl.BlockSpec(memory_space=VMEM)


def in_smem():
    return pl.BlockSpec(memory_space=SMEM)


def in_hbm():
    return pl.BlockSpec(memory_space=HBM)


def params(mib):
    return pltpu.CompilerParams(vmem_limit_bytes=mib << 20)


def cost(flops, moved):
    return pl.CostEstimate(flops=flops, bytes_accessed=moved, transcendentals=0)


def iota(shape, dim):
    return lax.broadcasted_iota(jnp.int32, shape, dim)


def dot(a, b):
    return jnp.dot(a, b, preferred_element_type=F32)


def dot_last(a, b):
    return lax.dot_general(a, b, (((1,), (1,)), ((), ())), preferred_element_type=F32)


def dot_first(a, b):
    return lax.dot_general(a, b, (((0,), (0,)), ((), ())), preferred_element_type=F32)


def norm_rows(floats, gain):
    center = jnp.mean(floats, -1, keepdims=True)
    shifted = floats - center
    spread = jnp.mean(jnp.square(shifted), -1, keepdims=True)
    return shifted * lax.rsqrt(spread + 1e-05) * gain


def split_high(values):
    high = values.astype(BF16)
    return high, values - high.astype(F32)


def chunked(src, dst, sems, index):
    size = dst.shape[0] // CHUNKS
    return [
        pltpu.make_async_copy(
            src.at[pl.ds(c * size, size)], dst.at[pl.ds(c * size, size)], sems.at[index, c]
        )
        for c in range(CHUNKS)
    ]


def start_all(copies):
    for copy in copies:
        copy.start()


def wait_all(copies):
    for copy in copies:
        copy.wait()


def attention_kernel(
    lengths, bias, tokens, gain, wq_hbm, k_hbm, v_hbm, wo_hbm, partial, wq, k, v, wo, sems
):
    copies = [
        chunked(src, dst, sems, i) for i, (src, dst) in enumerate(((wq_hbm, wq), (k_hbm, k), (v_hbm, v), (wo_hbm, wo)))
    ]
    start_all(copies[0] + copies[1])
    sequences = tokens.shape[0]
    heads = wq.shape[1] * 2 // LANES
    head_dim = LANES // 2
    length = k.shape[1]
    rows = heads * sequences
    wide = sequences * head_dim
    rounded = norm_rows(tokens[...].astype(F32), gain[...]).astype(BF16)
    wait_all(copies[0])
    start_all(copies[2] + copies[3])
    queries = dot(rounded, wq[...]).astype(BF16).astype(F32) * head_dim ** (-0.5)
    low_lane = iota((sequences, LANES), 1) < head_dim
    own_block = iota((sequences, wide), 1) // head_dim == iota((sequences, wide), 0)
    blocks = []
    for h in range(heads):
        slab = queries[:, h // 2 * LANES : (h // 2 + 1) * LANES]
        turned = pltpu.roll(slab, head_dim, 1)
        both = jnp.where(low_lane, slab, turned) if h % 2 == 0 else jnp.where(low_lane, turned, slab)
        blocks.append(jnp.where(own_block, jnp.concatenate([both] * (wide // LANES), axis=1), 0.0))
    spread_queries = jnp.concatenate(blocks, axis=0).astype(BF16)

    row = iota((rows, 1), 0)
    limit = jnp.zeros((rows, 1), jnp.int32)
    for s in range(sequences):
        limit = jnp.where(row % sequences == s, lengths[s], limit)
    offset = jnp.zeros((rows, 1), F32)
    for h in range(heads):
        offset = jnp.where(row // sequences == h, bias[h], offset)
    visible = iota((rows, length), 1) < limit

    wait_all(copies[1])
    scores = dot(spread_queries, k[...]) + offset
    tail = jnp.log1p(jnp.exp(-jnp.abs(scores)))
    keep = jnp.where(visible, -(jnp.maximum(scores, 0.0) + tail), 0.0)
    high, rest = split_high(keep)
    middle, rest = split_high(rest)
    low = rest.astype(BF16)
    span = 2 * LANES
    count = length // span
    pieces = [part[:, n * span : (n + 1) * span] for part in (high, middle, low) for n in range(count)]
    after = (iota((span, span), 0) > iota((span, span), 1)).astype(BF16)
    sums = dot(jnp.concatenate(pieces, axis=0), after)
    carry = jnp.zeros((rows, 1), F32)
    later = [None] * count
    for n in reversed(range(count)):
        within = (
            sums[n * rows : (n + 1) * rows]
            + sums[(count + n) * rows : (count + n + 1) * rows]
            + sums[(2 * count + n) * rows : (2 * count + n + 1) * rows]
        )
        later[n] = within + carry
        carry = carry + within[:, 0:1] + keep[:, n * span : n * span + 1]
    later_sum = jnp.concatenate(later, axis=1)
    stick = jnp.where(visible, jnp.exp(jnp.minimum(scores, 0.0) - tail + later_sum), 0.0).astype(BF16)

    wait_all(copies[2])
    mixed = dot_last(stick, v[...])
    own_rows = iota((rows, wide), 1) // head_dim == iota((rows, wide), 0) % sequences
    mixed = jnp.where(own_rows, mixed, 0.0)
    folded = mixed[:, 0:LANES]
    for j in range(1, wide // LANES):
        folded = folded + mixed[:, j * LANES : (j + 1) * LANES]
    folded = folded + pltpu.roll(folded, head_dim, 1)
    slabs = [
        jnp.where(
            low_lane,
            folded[h * sequences : (h + 1) * sequences],
            folded[(h + 1) * sequences : (h + 2) * sequences],
        )
        for h in range(0, heads, 2)
    ]
    attended = jnp.concatenate(slabs, axis=1).astype(BF16)
    wait_all(copies[3])
    partial[...] = dot(attended, wo[...])


def attention(tokens, gain, w_query, keys, values, lengths, bias, w_output):
    sequences, kv_local, head_dim, length = keys.shape
    assert kv_local == 1 and head_dim * 2 == LANES
    width = tokens.shape[1]
    wide = sequences * head_dim
    flat = (wide, length)
    return pl.pallas_call(
        attention_kernel,
        out_shape=jax.ShapeDtypeStruct((sequences, width), F32),
        in_specs=[in_smem(), in_smem(), in_vmem(), in_vmem()] + [in_hbm()] * 4,
        out_specs=in_vmem(),
        scratch_shapes=[
            VMEM(w_query.shape, BF16),
            VMEM(flat, BF16),
            VMEM(flat, BF16),
            VMEM(w_output.shape, BF16),
            pltpu.SemaphoreType.DMA((4, CHUNKS)),
        ],
        compiler_params=params(53),
        cost_estimate=cost(1 << 32, 7 << 20),
        name="attention",
    )(lengths, bias, tokens, gain.reshape(1, -1), w_query, keys.reshape(flat), values.reshape(flat), w_output)


def plan_kernel(capacity, routes, weights, partial, tokens, gain, place, share, base, normed):
    topk, sequences = routes.shape
    slots = place.shape[0]
    expert = iota((slots, sequences), 0) // capacity
    hit = jnp.zeros((slots, sequences), F32)
    weight = jnp.zeros((slots, sequences), F32)
    for j in range(topk):
        match = routes[j : j + 1, :] == expert
        hit = jnp.where(match, 1.0, hit)
        weight = jnp.where(match, weights[j : j + 1, :], weight)
    earlier = (iota((sequences, sequences), 0) < iota((sequences, sequences), 1)).astype(BF16)
    rank = dot(hit.astype(BF16), earlier)
    turn = (iota((slots, sequences), 0) % capacity).astype(F32)
    chosen = (hit > 0.0) & (rank == turn)
    place[...] = jnp.where(chosen, 1.0, 0.0).astype(BF16)
    share[...] = jnp.where(chosen, weight, 0.0)
    rounded = norm_rows(tokens[...].astype(F32), gain[...]).astype(BF16)
    normed[...] = rounded
    base[...] = rounded.astype(F32) + partial[...]


def plan(routes, route_weights, partial, tokens, gain, slots, capacity):
    sequences = routes.shape[0]
    return pl.pallas_call(
        functools.partial(plan_kernel, capacity),
        out_shape=(
            jax.ShapeDtypeStruct((slots, sequences), BF16),
            jax.ShapeDtypeStruct((slots, sequences), F32),
            jax.ShapeDtypeStruct(tokens.shape, F32),
            jax.ShapeDtypeStruct(tokens.shape, BF16),
        ),
        in_specs=[in_vmem()] * 5,
        out_specs=(in_vmem(),) * 4,
        compiler_params=params(8),
        cost_estimate=cost(1 << 20, 1 << 16),
        name="plan",
    )(jnp.transpose(routes), jnp.transpose(route_weights), partial, tokens, gain.reshape(1, -1))


def store_rows(scratch, values):
    count, width = values.shape
    parts = width // LANES
    for j in range(parts):
        scratch[pl.ds(j, count, stride=parts), :] = values[:, j * LANES : (j + 1) * LANES]


def load_rows(scratch, count):
    parts = scratch.shape[0] // count
    return jnp.concatenate(
        [scratch[pl.ds(j, count, stride=parts), :] for j in range(parts)], axis=1
    )


def half_of(ref, core, half):
    return ref[:, pl.ds(pl.multiple_of(core * half, half), half)]


def middle_kernel(base, other, gain, place, hidden, outgoing, scratch):
    half = base.shape[1] // 2
    hidden[...] = norm_rows(base[...] + other[...], gain[...]).astype(BF16)
    mine = half_of(hidden, lax.axis_index("tp"), half)
    store_rows(scratch, dot(place[...], mine))
    outgoing[...] = scratch[...].astype(BF16)


def middle(base, other, gain, place):
    sequences, width = base.shape
    packed = (place.shape[0] * (width // 2) // LANES, LANES)
    return pl.pallas_call(
        middle_kernel,
        out_shape=(
            jax.ShapeDtypeStruct((sequences, width), BF16),
            jax.ShapeDtypeStruct(packed, BF16),
        ),
        in_specs=[in_vmem()] * 4,
        out_specs=(in_vmem(), in_vmem()),
        scratch_shapes=[VMEM(packed, F32)],
        compiler_params=params(12),
        cost_estimate=cost(1 << 28, 1 << 20),
        name="middle",
    )(base, other, gain.reshape(1, -1), place)


def expert_kernel(own, other, gate, up, down, kept, sent, scratch, rows):
    core = lax.axis_index("tp")
    packed = own.shape[0]
    width = gate.shape[0]
    half = width // 2
    count = packed * LANES // half
    scratch[...] = own[...].astype(F32)
    own_rows = load_rows(scratch, count).astype(BF16)
    scratch[...] = other[...].astype(F32)
    other_rows = load_rows(scratch, count).astype(BF16)
    rows[:, pl.ds(pl.multiple_of(core * half, half), half)] = own_rows
    rows[:, pl.ds(pl.multiple_of((1 - core) * half, half), half)] = other_rows
    inputs = rows[...]
    gate_pre = dot(inputs, gate[...])
    up_pre = dot(inputs, up[...])
    act = (jax.nn.silu(gate_pre) * up_pre).astype(BF16)
    store_rows(scratch, dot(act, half_of(down, core, half)))
    kept[...] = scratch[...].astype(BF16)
    store_rows(scratch, dot(act, half_of(down, 1 - core, half)))
    sent[...] = scratch[...].astype(BF16)


def expert(own, other, gate, up, down):
    packed = own.shape
    width = gate.shape[0]
    count = packed[0] * LANES * 2 // width
    return pl.pallas_call(
        expert_kernel,
        out_shape=(jax.ShapeDtypeStruct(packed, BF16), jax.ShapeDtypeStruct(packed, BF16)),
        in_specs=[in_vmem()] * 5,
        out_specs=(in_vmem(), in_vmem()),
        scratch_shapes=[VMEM(packed, F32), VMEM((count, width), BF16)],
        compiler_params=params(24),
        cost_estimate=cost(1 << 30, 4 << 20),
        name="expert",
    )(own, other, gate, up, down)


def fetch_kernel(*refs):
    count = len(refs) // 2
    sources, targets, sems = refs[:count], refs[count : 2 * count], refs[-1]
    copies = [chunked(src, dst, sems, i) for i, (src, dst) in enumerate(zip(sources, targets))]
    for group in copies:
        start_all(group)
    for group in copies:
        wait_all(group)


def fetch(*weights):
    return pl.pallas_call(
        fetch_kernel,
        out_shape=tuple(jax.ShapeDtypeStruct(w.shape, w.dtype) for w in weights),
        in_specs=[in_hbm()] * len(weights),
        out_specs=tuple(in_vmem() for _ in weights),
        scratch_shapes=[pltpu.SemaphoreType.DMA((len(weights), CHUNKS))],
        compiler_params=params(49),
        cost_estimate=cost(1 << 28, 6 << 20),
        name="fetch",
    )(*weights)


def add_kernel(a, b, out):
    out[...] = (a[...].astype(F32) + b[...].astype(F32)).astype(BF16)


def add_rounded(a, b):
    return pl.pallas_call(
        add_kernel,
        out_shape=jax.ShapeDtypeStruct(a.shape, BF16),
        in_specs=[in_vmem()] * 2,
        out_specs=in_vmem(),
        compiler_params=params(4),
        cost_estimate=cost(1 << 18, 1 << 19),
        name="add_parts",
    )(a, b)


def combine_kernel(returned, share, out, scratch):
    scratch[...] = returned[...].astype(F32)
    rows = load_rows(scratch, share.shape[0]).astype(BF16)
    high, rest = split_high(share[...])
    out[...] = dot_first(high, rows) + dot_first(rest.astype(BF16), rows)


def combine(returned, share):
    half = returned.shape[0] * LANES // share.shape[0]
    return pl.pallas_call(
        combine_kernel,
        out_shape=jax.ShapeDtypeStruct((share.shape[1], half), F32),
        in_specs=[in_vmem()] * 2,
        out_specs=in_vmem(),
        scratch_shapes=[VMEM(returned.shape, F32)],
        compiler_params=params(8),
        cost_estimate=cost(1 << 24, 1 << 19),
        name="combine",
    )(returned, share)


def last_kernel(own, other, dense, dense_other, hidden, mix_gate, gain, mixed, total):
    core = lax.axis_index("tp")
    half = own.shape[1]
    floats = hidden[...].astype(F32)
    mix = jax.nn.sigmoid(jnp.sum(floats * mix_gate[...], axis=-1, keepdims=True))
    total[...] = floats + mix * (dense[...] + dense_other[...])
    mine = pl.ds(pl.multiple_of(core * half, half), half)
    theirs = pl.ds(pl.multiple_of((1 - core) * half, half), half)
    total[:, mine] = total[:, mine] + own[...]
    total[:, theirs] = total[:, theirs] + other[...]
    mixed[...] = norm_rows(total[...], gain[...]).astype(BF16)


def last(own, other, dense, dense_other, hidden, mix_gate, gain):
    return pl.pallas_call(
        last_kernel,
        out_shape=jax.ShapeDtypeStruct(hidden.shape, BF16),
        in_specs=[in_vmem()] * 7,
        out_specs=in_vmem(),
        scratch_shapes=[VMEM(hidden.shape, F32)],
        compiler_params=params(8),
        cost_estimate=cost(1 << 20, 1 << 20),
        name="last",
    )(own, other, dense, dense_other, hidden, mix_gate.reshape(1, -1), gain.reshape(1, -1))


def fresh_kernel(normed, w_key, w_value, keys, values):
    rows = normed[...]
    keys[...] = dot_last(rows, w_key[...]).astype(BF16)
    values[...] = dot_last(rows, w_value[...]).astype(BF16)


def fresh(normed, w_key, w_value):
    shape = jax.ShapeDtypeStruct((normed.shape[0], w_key.shape[1]), BF16)
    return pl.pallas_call(
        fresh_kernel,
        out_shape=(shape, shape),
        in_specs=[in_vmem()] * 3,
        out_specs=(in_vmem(), in_vmem()),
        compiler_params=params(8),
        cost_estimate=cost(1 << 24, 1 << 19),
        name="fresh",
    )(normed, jnp.transpose(w_key), jnp.transpose(w_value))


def swap_core(values):
    return lax.ppermute(values, "tp", [(0, 1), (1, 0)])


def exchange(packed, ep_count):
    blocks = packed.reshape(ep_count, -1, LANES)
    moved = lax.all_to_all(blocks, "ep", split_axis=0, concat_axis=0, tiled=True)
    return moved.reshape(packed.shape)


def swap_far(values, bit):
    count = lax.axis_size("ep")
    return lax.ppermute(values, "ep", [(i, i ^ bit) for i in range(count)])


def pack_kernel(gate_hbm, up_hbm, down_hbm, packed, gate, up, down, sems):
    copies = [
        pltpu.make_async_copy(src, dst, sems.at[i])
        for i, (src, dst) in enumerate(((gate_hbm, gate), (up_hbm, up), (down_hbm, down)))
    ]
    start_all(copies)
    wait_all(copies)
    core = lax.axis_index("tp")
    rows, units = gate.shape
    share = units // 2
    packed[0:rows, 0:share] = half_of(gate, core, share)
    packed[0:rows, share:units] = half_of(up, core, share)
    mine = down[pl.ds(pl.multiple_of(core * share, share), share), :]
    packed[rows:, 0:share] = mine[0 : share // 2]
    packed[rows:, share:units] = mine[share // 2 : share]


def pack(gate, up, down):
    rows, units = gate.shape
    return pl.pallas_call(
        pack_kernel,
        out_shape=jax.ShapeDtypeStruct((rows + units // 4, units), BF16),
        in_specs=[in_hbm()] * 3,
        out_specs=in_vmem(),
        scratch_shapes=[
            VMEM(gate.shape, BF16),
            VMEM(up.shape, BF16),
            VMEM(down.shape, BF16),
            pltpu.SemaphoreType.DMA((3,)),
        ],
        compiler_params=pltpu.CompilerParams(vmem_limit_bytes=(53 << 20) + (10240 << 10)),
        cost_estimate=cost(1 << 32, 1 << 18),
        name="pack",
    )(gate, up, down)


def join_kernel(*refs):
    out, at = refs[-1], 0
    for ref in refs[:-1]:
        out[at : at + ref.shape[0], :] = ref[...]
        at += ref.shape[0]


def join(*blocks):
    rows = sum(block.shape[0] for block in blocks)
    return pl.pallas_call(
        join_kernel,
        out_shape=jax.ShapeDtypeStruct((rows, blocks[0].shape[1]), BF16),
        in_specs=[in_vmem()] * len(blocks),
        out_specs=in_vmem(),
        compiler_params=params(8),
        cost_estimate=cost(1 << 18, 1 << 19),
        name="join",
    )(*blocks)


def dense_kernel(offsets, hidden, *refs):
    sources, out = refs[:-1], refs[-1]
    units = sources[0].shape[1]
    share = units // 2
    rows = LANES
    height = rows + share // 2
    me = lax.axis_index("ep")
    blocks = []
    for ref, group in zip(sources, offsets):
        for n, offset in enumerate(group):
            blocks.append((ref, n * height, (me ^ offset) * rows))
    pre = jnp.zeros((hidden.shape[0], units), F32)
    for j in range(0, len(blocks), 2):
        left = [hidden[:, pl.ds(pl.multiple_of(at, rows), rows)] for _, _, at in blocks[j : j + 2]]
        right = [ref[start : start + rows, :] for ref, start, _ in blocks[j : j + 2]]
        pre = pre + dot(jnp.concatenate(left, axis=1), jnp.concatenate(right, axis=0))
    act = (jax.nn.silu(pre[:, 0:share]) * pre[:, share:units]).astype(BF16)
    for ref, start, at in blocks:
        tail = ref[start + rows : start + height, :]
        down = jnp.concatenate([tail[:, 0:share], tail[:, share:units]], axis=0)
        out[:, pl.ds(pl.multiple_of(at, rows), rows)] = dot(act, down)


def dense(hidden, sources, offsets):
    return pl.pallas_call(
        functools.partial(dense_kernel, offsets),
        out_shape=jax.ShapeDtypeStruct(hidden.shape, F32),
        in_specs=[in_vmem()] * (1 + len(sources)),
        out_specs=in_vmem(),
        compiler_params=params(8),
        cost_estimate=cost(1 << 28, 2 << 20),
        name="dense",
    )(hidden, *sources)


def dense_weights(dense_gate, dense_up, dense_down):
    share = dense_gate.shape[1] // lax.axis_size("tp")
    offset = lax.axis_index("tp") * share
    gate = lax.dynamic_slice_in_dim(dense_gate, offset, share, 1)
    up = lax.dynamic_slice_in_dim(dense_up, offset, share, 1)
    down = lax.dynamic_slice_in_dim(dense_down, offset, share, 0)
    return jnp.concatenate(
        [gate.reshape(-1, LANES), up.reshape(-1, LANES), down.reshape(-1, LANES)]
    )


def dense_narrow(hidden, packed, rows, share):
    count = lax.axis_size("ep")
    packed = packed[None]
    bits = [count >> (n + 1) for n in range(count.bit_length() - 1)]
    for bit in bits:
        packed = jnp.concatenate([packed, swap_far(packed, bit)])
    order = [0] * count
    for j in range(count):
        order[sum(bit for n, bit in enumerate(bits) if j >> n & 1)] = j
    packed = jnp.take(packed[jnp.array(order)], lax.axis_index("ep") ^ jnp.arange(count), axis=0)
    packed = packed.reshape(count, 3, rows * share)
    gate = packed[:, 0].reshape(count * rows, share)
    up = packed[:, 1].reshape(count * rows, share)
    down = jnp.moveaxis(packed[:, 2].reshape(count, share, rows), 0, 1).reshape(share, -1)
    act = (jax.nn.silu(dot(hidden, gate)) * dot(hidden, up)).astype(BF16)
    return dot(act, down)


def shards(
    tokens,
    cache_keys,
    cache_values,
    cache_lengths,
    norm_in,
    w_query,
    w_key,
    w_value,
    stick_bias,
    w_output,
    norm_mid,
    routes,
    route_weights,
    expert_gate,
    expert_up,
    expert_down,
    dense_gate,
    dense_up,
    dense_down,
    mix_gate,
    norm_out,
):
    sequences, topk = routes.shape
    ep_count = lax.axis_size("ep")
    experts = ep_count * expert_gate.shape[0]
    capacity = max(2, (sequences * topk + ep_count - 1) // ep_count)
    slots = experts * capacity
    rows = dense_gate.shape[0]
    share = dense_gate.shape[1] // lax.axis_size("tp")
    wide = rows == LANES and share == LANES
    if wide:
        block = pack(dense_gate, dense_up, dense_down)
        columns = [0]
        bit = ep_count // 2
        far = []
        while bit > 2:
            far.append(swap_far(block, bit))
            columns = columns + [c ^ bit for c in columns]
            if bit > 4 or bit == 4:
                block = join(block, far[-1])
            bit //= 2
    partial = attention(
        tokens, norm_in, w_query, cache_keys, cache_values, cache_lengths, stick_bias, w_output
    )
    place, portion, base, normed = plan(
        routes, route_weights, partial, tokens, norm_in, slots, capacity
    )
    partial_other = swap_core(partial)
    hidden, outgoing = middle(base, partial_other, norm_mid, place)
    received = exchange(outgoing, ep_count)
    received_other = swap_core(received)
    weights = fetch(expert_gate[0], expert_up[0], expert_down[0])
    kept, sent = expert(received, received_other, *weights)
    sent_other = swap_core(sent)
    summed = add_rounded(kept, sent_other)
    returned = exchange(summed, ep_count)
    fresh_keys, fresh_values = fresh(normed, w_key, w_value)
    if wide:
        from_x = swap_far(block, 1)
        from_y = swap_far(block, 2)
        part = block.shape[0] // 2
        diagonal_low = swap_far(from_y[:part], 1)
        diagonal_high = swap_far(from_x[part:], 2)
        count = len(columns) // 2
        offsets = (
            tuple(columns),
            tuple(c ^ 1 for c in columns),
            tuple(c ^ 2 for c in columns),
            tuple(c ^ 3 for c in columns[:count]),
            tuple(c ^ 3 for c in columns[count:]),
        )
        dense_out = dense(hidden, (block, from_x, from_y, diagonal_low, diagonal_high), offsets)
    else:
        packed = dense_weights(dense_gate, dense_up, dense_down)
        dense_out = dense_narrow(hidden, packed, rows, share)
    dense_other = swap_core(dense_out)
    own = combine(returned, portion)
    own_other = swap_core(own)
    mixed = last(own, own_other, dense_out, dense_other, hidden, mix_gate, norm_out)
    return (mixed, fresh_keys, fresh_values)


def solution(mesh):
    in_specs = (
        P("ep", None),
        P("ep", "tp", None, None),
        P("ep", "tp", None, None),
        P("ep"),
        P(),
        P(None, "tp"),
        P(None, "tp"),
        P(None, "tp"),
        P("tp"),
        P("tp", None),
        P(),
        P("ep", None),
        P("ep", None),
        P("ep", None, "tp"),
        P("ep", None, "tp"),
        P("ep", "tp", None),
        P("ep", None),
        P("ep", None),
        P(None, "ep"),
        P(),
        P(),
    )
    out_specs = (P("ep", None), P("ep", "tp"), P("ep", "tp"))
    return jax.shard_map(shards, mesh=mesh, in_specs=in_specs, out_specs=out_specs, check_vma=False)
```

```python
import functools

import jax
import jax.numpy as jnp
from jax import lax
from jax.experimental import pallas as pl
from jax.experimental.pallas import tpu as pltpu
from jax.sharding import PartitionSpec as P


LANES = 128
CHUNKS = 2
F32 = jnp.float32
BF16 = jnp.bfloat16
VMEM = pltpu.VMEM
SMEM = pltpu.SMEM
HBM = pltpu.MemorySpace.HBM


def in_vmem():
    return pl.BlockSpec(memory_space=VMEM)


def in_smem():
    return pl.BlockSpec(memory_space=SMEM)


def in_hbm():
    return pl.BlockSpec(memory_space=HBM)


def params(mib):
    return pltpu.CompilerParams(vmem_limit_bytes=mib << 20)


def cost(flops, moved):
    return pl.CostEstimate(flops=flops, bytes_accessed=moved, transcendentals=0)


def iota(shape, dim):
    return lax.broadcasted_iota(jnp.int32, shape, dim)


def dot(a, b):
    return jnp.dot(a, b, preferred_element_type=F32)


def dot_last(a, b):
    return lax.dot_general(a, b, (((1,), (1,)), ((), ())), preferred_element_type=F32)


def dot_first(a, b):
    return lax.dot_general(a, b, (((0,), (0,)), ((), ())), preferred_element_type=F32)


def norm_rows(floats, gain):
    center = jnp.mean(floats, -1, keepdims=True)
    shifted = floats - center
    spread = jnp.mean(jnp.square(shifted), -1, keepdims=True)
    return shifted * lax.rsqrt(spread + 1e-05) * gain


def split_high(values):
    high = values.astype(BF16)
    return high, values - high.astype(F32)


def chunked(src, dst, sems, index):
    size = dst.shape[0] // CHUNKS
    return [
        pltpu.make_async_copy(
            src.at[pl.ds(c * size, size)], dst.at[pl.ds(c * size, size)], sems.at[index, c]
        )
        for c in range(CHUNKS)
    ]


def start_all(copies):
    for copy in copies:
        copy.start()


def wait_all(copies):
    for copy in copies:
        copy.wait()


def plan_slots(capacity, routes, weights, place, share):
    topk, sequences = routes.shape
    slots = place.shape[0]
    expert = iota((slots, sequences), 0) // capacity
    hit = jnp.zeros((slots, sequences), F32)
    weight = jnp.zeros((slots, sequences), F32)
    for j in range(topk):
        match = routes[j : j + 1, :] == expert
        hit = jnp.where(match, 1.0, hit)
        weight = jnp.where(match, weights[j : j + 1, :], weight)
    earlier = (iota((sequences, sequences), 0) < iota((sequences, sequences), 1)).astype(BF16)
    rank = dot(hit.astype(BF16), earlier)
    turn = (iota((slots, sequences), 0) % capacity).astype(F32)
    chosen = (hit > 0.0) & (rank == turn)
    place[...] = jnp.where(chosen, 1.0, 0.0).astype(BF16)
    share[...] = jnp.where(chosen, weight, 0.0)


def attention_kernel(
    capacity,
    lengths,
    bias,
    tokens,
    gain,
    routes,
    weights,
    wq_hbm,
    k_hbm,
    v_hbm,
    wo_hbm,
    partial,
    normed,
    place,
    share,
    wq,
    k,
    v,
    wo,
    sems,
):
    copies = [
        chunked(src, dst, sems, i) for i, (src, dst) in enumerate(((wq_hbm, wq), (k_hbm, k), (v_hbm, v), (wo_hbm, wo)))
    ]
    start_all(copies[0] + copies[1])
    sequences = tokens.shape[0]
    heads = wq.shape[1] * 2 // LANES
    head_dim = LANES // 2
    length = k.shape[1]
    rows = heads * sequences
    wide = sequences * head_dim
    rounded = norm_rows(tokens[...].astype(F32), gain[...]).astype(BF16)
    normed[...] = rounded
    plan_slots(capacity, routes, weights, place, share)
    wait_all(copies[0])
    start_all(copies[2] + copies[3])
    queries = dot(rounded, wq[...]).astype(BF16).astype(F32) * head_dim ** (-0.5)
    low_lane = iota((sequences, LANES), 1) < head_dim
    own_block = iota((sequences, wide), 1) // head_dim == iota((sequences, wide), 0)
    blocks = []
    for h in range(heads):
        slab = queries[:, h // 2 * LANES : (h // 2 + 1) * LANES]
        turned = pltpu.roll(slab, head_dim, 1)
        both = jnp.where(low_lane, slab, turned) if h % 2 == 0 else jnp.where(low_lane, turned, slab)
        blocks.append(jnp.where(own_block, jnp.concatenate([both] * (wide // LANES), axis=1), 0.0))
    spread_queries = jnp.concatenate(blocks, axis=0).astype(BF16)

    row = iota((rows, 1), 0)
    limit = jnp.zeros((rows, 1), jnp.int32)
    for s in range(sequences):
        limit = jnp.where(row % sequences == s, lengths[s], limit)
    offset = jnp.zeros((rows, 1), F32)
    for h in range(heads):
        offset = jnp.where(row // sequences == h, bias[h], offset)
    visible = iota((rows, length), 1) < limit

    wait_all(copies[1])
    scores = dot(spread_queries, k[...]) + offset
    tail = jnp.log1p(jnp.exp(-jnp.abs(scores)))
    keep = jnp.where(visible, -(jnp.maximum(scores, 0.0) + tail), 0.0)
    high, rest = split_high(keep)
    middle, rest = split_high(rest)
    low = rest.astype(BF16)
    span = 2 * LANES
    count = length // span
    pieces = [part[:, n * span : (n + 1) * span] for part in (high, middle, low) for n in range(count)]
    after = (iota((span, span), 0) > iota((span, span), 1)).astype(BF16)
    sums = dot(jnp.concatenate(pieces, axis=0), after)
    carry = jnp.zeros((rows, 1), F32)
    later = [None] * count
    for n in reversed(range(count)):
        within = (
            sums[n * rows : (n + 1) * rows]
            + sums[(count + n) * rows : (count + n + 1) * rows]
            + sums[(2 * count + n) * rows : (2 * count + n + 1) * rows]
        )
        later[n] = within + carry
        carry = carry + within[:, 0:1] + keep[:, n * span : n * span + 1]
    later_sum = jnp.concatenate(later, axis=1)
    stick = jnp.where(visible, jnp.exp(jnp.minimum(scores, 0.0) - tail + later_sum), 0.0).astype(BF16)

    wait_all(copies[2])
    mixed = dot_last(stick, v[...])
    own_rows = iota((rows, wide), 1) // head_dim == iota((rows, wide), 0) % sequences
    mixed = jnp.where(own_rows, mixed, 0.0)
    folded = mixed[:, 0:LANES]
    for j in range(1, wide // LANES):
        folded = folded + mixed[:, j * LANES : (j + 1) * LANES]
    folded = folded + pltpu.roll(folded, head_dim, 1)
    slabs = [
        jnp.where(
            low_lane,
            folded[h * sequences : (h + 1) * sequences],
            folded[(h + 1) * sequences : (h + 2) * sequences],
        )
        for h in range(0, heads, 2)
    ]
    attended = jnp.concatenate(slabs, axis=1).astype(BF16)
    wait_all(copies[3])
    partial[...] = dot(attended, wo[...])


def attention(
    tokens, gain, w_query, keys, values, lengths, bias, w_output, routes, weights, slots, capacity
):
    sequences, kv_local, head_dim, length = keys.shape
    assert kv_local == 1 and head_dim * 2 == LANES
    width = tokens.shape[1]
    wide = sequences * head_dim
    flat = (wide, length)
    return pl.pallas_call(
        functools.partial(attention_kernel, capacity),
        out_shape=(
            jax.ShapeDtypeStruct((sequences, width), F32),
            jax.ShapeDtypeStruct((sequences, width), BF16),
            jax.ShapeDtypeStruct((slots, sequences), BF16),
            jax.ShapeDtypeStruct((slots, sequences), F32),
        ),
        in_specs=[in_smem()] * 2 + [in_vmem()] * 4 + [in_hbm()] * 4,
        out_specs=(in_vmem(),) * 4,
        scratch_shapes=[
            VMEM(w_query.shape, BF16),
            VMEM(flat, BF16),
            VMEM(flat, BF16),
            VMEM(w_output.shape, BF16),
            pltpu.SemaphoreType.DMA((4, CHUNKS)),
        ],
        compiler_params=params(53),
        cost_estimate=cost(1 << 32, 7 << 20),
        name="attention",
    )(
        lengths,
        bias,
        tokens,
        gain.reshape(1, -1),
        jnp.transpose(routes),
        jnp.transpose(weights),
        w_query,
        keys.reshape(flat),
        values.reshape(flat),
        w_output,
    )


def store_rows(scratch, values):
    count, width = values.shape
    parts = width // LANES
    for j in range(parts):
        scratch[pl.ds(j, count, stride=parts), :] = values[:, j * LANES : (j + 1) * LANES]


def load_rows(scratch, count):
    parts = scratch.shape[0] // count
    return jnp.concatenate(
        [scratch[pl.ds(j, count, stride=parts), :] for j in range(parts)], axis=1
    )


def half_of(ref, core, half):
    return ref[:, pl.ds(pl.multiple_of(core * half, half), half)]


def middle_kernel(partial, other, normed, gain, place, hidden, outgoing, scratch):
    half = partial.shape[1] // 2
    floats = normed[...].astype(F32) + (partial[...] + other[...])
    hidden[...] = norm_rows(floats, gain[...]).astype(BF16)
    mine = half_of(hidden, lax.axis_index("tp"), half)
    store_rows(scratch, dot(place[...], mine))
    outgoing[...] = scratch[...].astype(BF16)


def middle(partial, other, normed, gain, place):
    sequences, width = partial.shape
    packed = (place.shape[0] * (width // 2) // LANES, LANES)
    return pl.pallas_call(
        middle_kernel,
        out_shape=(
            jax.ShapeDtypeStruct((sequences, width), BF16),
            jax.ShapeDtypeStruct(packed, BF16),
        ),
        in_specs=[in_vmem()] * 5,
        out_specs=(in_vmem(), in_vmem()),
        scratch_shapes=[VMEM(packed, F32)],
        compiler_params=params(12),
        cost_estimate=cost(1 << 28, 1 << 20),
        name="middle",
    )(partial, other, normed, gain.reshape(1, -1), place)


def first_kernel(own, gate_hbm, up_hbm, down_hbm, pre, gate, up, down, scratch, gate_own, up_own, sems):
    core = lax.axis_index("tp")
    half = gate.shape[0]
    mine = pl.ds(pl.multiple_of(core * half, half), half)
    theirs = pl.ds(pl.multiple_of((1 - core) * half, half), half)
    early = chunked(gate_hbm.at[mine], gate_own, sems, 0) + chunked(up_hbm.at[mine], up_own, sems, 1)
    late = chunked(gate_hbm.at[theirs], gate, sems, 2) + chunked(up_hbm.at[theirs], up, sems, 3)
    late = late + chunked(down_hbm, down, sems, 4)
    start_all(early + late)
    scratch[...] = own[...].astype(F32)
    rows = load_rows(scratch, pre.shape[0]).astype(BF16)
    wait_all(early)
    units = gate.shape[1]
    pre[:, 0:units] = dot(rows, gate_own[...])
    pre[:, units:] = dot(rows, up_own[...])
    wait_all(late)


def expert_first(own, gate, up, down):
    packed = own.shape
    width, units = gate.shape
    half = width // 2
    count = packed[0] * LANES // half
    part = jax.ShapeDtypeStruct((half, units), BF16)
    return pl.pallas_call(
        first_kernel,
        out_shape=(
            jax.ShapeDtypeStruct((count, 2 * units), F32),
            part,
            part,
            jax.ShapeDtypeStruct(down.shape, BF16),
        ),
        in_specs=[in_vmem()] + [in_hbm()] * 3,
        out_specs=(in_vmem(),) * 4,
        scratch_shapes=[
            VMEM(packed, F32),
            VMEM(part.shape, BF16),
            VMEM(part.shape, BF16),
            pltpu.SemaphoreType.DMA((5, CHUNKS)),
        ],
        compiler_params=params(50),
        cost_estimate=cost(1 << 28, 4 << 20),
        name="expert_first",
    )(own, gate, up, down)


def second_kernel(other, pre, gate, up, down, sent, act_out, scratch):
    core = lax.axis_index("tp")
    units = gate.shape[1]
    half = down.shape[1] // 2
    scratch[...] = other[...].astype(F32)
    rows = load_rows(scratch, pre.shape[0]).astype(BF16)
    gate_pre = pre[:, 0:units] + dot(rows, gate[...])
    up_pre = pre[:, units:] + dot(rows, up[...])
    act = (jax.nn.silu(gate_pre) * up_pre).astype(BF16)
    act_out[...] = act
    store_rows(scratch, dot(act, half_of(down, 1 - core, half)))
    sent[...] = scratch[...].astype(BF16)


def expert_second(other, pre, gate, up, down):
    packed = other.shape
    return pl.pallas_call(
        second_kernel,
        out_shape=(
            jax.ShapeDtypeStruct(packed, BF16),
            jax.ShapeDtypeStruct((pre.shape[0], gate.shape[1]), BF16),
        ),
        in_specs=[in_vmem()] * 5,
        out_specs=(in_vmem(), in_vmem()),
        scratch_shapes=[VMEM(packed, F32)],
        compiler_params=params(16),
        cost_estimate=cost(1 << 28, 2 << 20),
        name="expert_second",
    )(other, pre, gate, up, down)


def third_kernel(act, down, kept, scratch):
    half = down.shape[1] // 2
    store_rows(scratch, dot(act[...], half_of(down, lax.axis_index("tp"), half)))
    kept[...] = scratch[...].astype(BF16)


def expert_third(act, down):
    packed = (act.shape[0] * down.shape[1] // 2 // LANES, LANES)
    return pl.pallas_call(
        third_kernel,
        out_shape=jax.ShapeDtypeStruct(packed, BF16),
        in_specs=[in_vmem()] * 2,
        out_specs=in_vmem(),
        scratch_shapes=[VMEM(packed, F32)],
        compiler_params=params(16),
        cost_estimate=cost(1 << 26, 2 << 20),
        name="expert_third",
    )(act, down)


def add_kernel(a, b, out):
    out[...] = (a[...].astype(F32) + b[...].astype(F32)).astype(BF16)


def add_rounded(a, b):
    return pl.pallas_call(
        add_kernel,
        out_shape=jax.ShapeDtypeStruct(a.shape, BF16),
        in_specs=[in_vmem()] * 2,
        out_specs=in_vmem(),
        compiler_params=params(4),
        cost_estimate=cost(1 << 18, 1 << 19),
        name="add_parts",
    )(a, b)


def combine_kernel(returned, share, out, scratch):
    scratch[...] = returned[...].astype(F32)
    rows = load_rows(scratch, share.shape[0]).astype(BF16)
    high, rest = split_high(share[...])
    out[...] = dot_first(high, rows) + dot_first(rest.astype(BF16), rows)


def combine(returned, share):
    half = returned.shape[0] * LANES // share.shape[0]
    return pl.pallas_call(
        combine_kernel,
        out_shape=jax.ShapeDtypeStruct((share.shape[1], half), F32),
        in_specs=[in_vmem()] * 2,
        out_specs=in_vmem(),
        scratch_shapes=[VMEM(returned.shape, F32)],
        compiler_params=params(8),
        cost_estimate=cost(1 << 24, 1 << 19),
        name="combine",
    )(returned, share)


def last_kernel(own, other, dense, dense_other, hidden, mix_gate, gain, mixed, total):
    core = lax.axis_index("tp")
    half = own.shape[1]
    floats = hidden[...].astype(F32)
    mix = jax.nn.sigmoid(jnp.sum(floats * mix_gate[...], axis=-1, keepdims=True))
    total[...] = floats + mix * (dense[...] + dense_other[...])
    mine = pl.ds(pl.multiple_of(core * half, half), half)
    theirs = pl.ds(pl.multiple_of((1 - core) * half, half), half)
    total[:, mine] = total[:, mine] + own[...]
    total[:, theirs] = total[:, theirs] + other[...]
    mixed[...] = norm_rows(total[...], gain[...]).astype(BF16)


def last(own, other, dense, dense_other, hidden, mix_gate, gain):
    return pl.pallas_call(
        last_kernel,
        out_shape=jax.ShapeDtypeStruct(hidden.shape, BF16),
        in_specs=[in_vmem()] * 7,
        out_specs=in_vmem(),
        scratch_shapes=[VMEM(hidden.shape, F32)],
        compiler_params=params(8),
        cost_estimate=cost(1 << 20, 1 << 20),
        name="last",
    )(own, other, dense, dense_other, hidden, mix_gate.reshape(1, -1), gain.reshape(1, -1))


def fresh_kernel(normed, w_key, w_value, keys, values):
    rows = normed[...]
    keys[...] = dot_last(rows, w_key[...]).astype(BF16)
    values[...] = dot_last(rows, w_value[...]).astype(BF16)


def fresh(normed, w_key, w_value):
    shape = jax.ShapeDtypeStruct((normed.shape[0], w_key.shape[1]), BF16)
    return pl.pallas_call(
        fresh_kernel,
        out_shape=(shape, shape),
        in_specs=[in_vmem()] * 3,
        out_specs=(in_vmem(), in_vmem()),
        compiler_params=params(8),
        cost_estimate=cost(1 << 24, 1 << 19),
        name="fresh",
    )(normed, jnp.transpose(w_key), jnp.transpose(w_value))


def swap_core(values):
    return lax.ppermute(values, "tp", [(0, 1), (1, 0)])


def exchange(packed, ep_count):
    blocks = packed.reshape(ep_count, -1, LANES)
    moved = lax.all_to_all(blocks, "ep", split_axis=0, concat_axis=0, tiled=True)
    return moved.reshape(packed.shape)


def swap_far(values, bit):
    count = lax.axis_size("ep")
    return lax.ppermute(values, "ep", [(i, i ^ bit) for i in range(count)])


def pack_kernel(gate_hbm, up_hbm, down_hbm, packed, gate, up, down, sems):
    copies = [
        pltpu.make_async_copy(src, dst, sems.at[i])
        for i, (src, dst) in enumerate(((gate_hbm, gate), (up_hbm, up), (down_hbm, down)))
    ]
    start_all(copies)
    wait_all(copies)
    core = lax.axis_index("tp")
    rows, units = gate.shape
    share = units // 2
    packed[0:rows, 0:share] = half_of(gate, core, share)
    packed[0:rows, share:units] = half_of(up, core, share)
    mine = down[pl.ds(pl.multiple_of(core * share, share), share), :]
    packed[rows:, 0:share] = mine[0 : share // 2]
    packed[rows:, share:units] = mine[share // 2 : share]


def pack(gate, up, down):
    rows, units = gate.shape
    return pl.pallas_call(
        pack_kernel,
        out_shape=jax.ShapeDtypeStruct((rows + units // 4, units), BF16),
        in_specs=[in_hbm()] * 3,
        out_specs=in_vmem(),
        scratch_shapes=[
            VMEM(gate.shape, BF16),
            VMEM(up.shape, BF16),
            VMEM(down.shape, BF16),
            pltpu.SemaphoreType.DMA((3,)),
        ],
        compiler_params=params(63),
        cost_estimate=cost(1 << 32, 1 << 18),
        name="pack",
    )(gate, up, down)


def join_kernel(*refs):
    out, at = refs[-1], 0
    for ref in refs[:-1]:
        out[at : at + ref.shape[0], :] = ref[...]
        at += ref.shape[0]


def join(*blocks):
    rows = sum(block.shape[0] for block in blocks)
    return pl.pallas_call(
        join_kernel,
        out_shape=jax.ShapeDtypeStruct((rows, blocks[0].shape[1]), BF16),
        in_specs=[in_vmem()] * len(blocks),
        out_specs=in_vmem(),
        compiler_params=params(8),
        cost_estimate=cost(1 << 18, 1 << 19),
        name="join",
    )(*blocks)


def slabs_of(sources, offsets):
    height = LANES + sources[0].shape[1] // 4
    me = lax.axis_index("ep")
    return [
        (ref, n * height, pl.ds(pl.multiple_of((me ^ offset) * LANES, LANES), LANES))
        for ref, group in zip(sources, offsets)
        for n, offset in enumerate(group)
    ]


def add_slabs(pre, hidden, slabs):
    for j in range(0, len(slabs), 2):
        left = [hidden[:, at] for _, _, at in slabs[j : j + 2]]
        right = [ref[start : start + LANES, :] for ref, start, _ in slabs[j : j + 2]]
        pre = pre + dot(jnp.concatenate(left, axis=1), jnp.concatenate(right, axis=0))
    return pre


def early_kernel(offsets, hidden, *refs):
    sources, out = refs[:-1], refs[-1]
    out[...] = add_slabs(jnp.zeros(out.shape, F32), hidden, slabs_of(sources, offsets))


def dense_early(hidden, sources, offsets):
    return pl.pallas_call(
        functools.partial(early_kernel, offsets),
        out_shape=jax.ShapeDtypeStruct((hidden.shape[0], sources[0].shape[1]), F32),
        in_specs=[in_vmem()] * (1 + len(sources)),
        out_specs=in_vmem(),
        compiler_params=params(8),
        cost_estimate=cost(1 << 26, 1 << 20),
        name="dense_early",
    )(hidden, *sources)


def dense_kernel(late, offsets, hidden, early, *refs):
    sources, out = refs[:-1], refs[-1]
    share = early.shape[1] // 2
    slabs = slabs_of(sources, offsets)
    count = sum(len(group) for group in offsets[:late])
    pre = add_slabs(early[...], hidden, slabs[:count])
    act = (jax.nn.silu(pre[:, 0:share]) * pre[:, share:]).astype(BF16)
    for j in range(0, len(slabs), 2):
        downs = []
        for ref, start, _ in slabs[j : j + 2]:
            tail = ref[start + LANES : start + LANES + share // 2, :]
            downs.append(jnp.concatenate([tail[:, 0:share], tail[:, share:]], axis=0))
        both = dot(act, jnp.concatenate(downs, axis=1))
        for n, (_, _, at) in enumerate(slabs[j : j + 2]):
            out[:, at] = both[:, n * LANES : (n + 1) * LANES]


def dense(hidden, early, late, sources, offsets):
    return pl.pallas_call(
        functools.partial(dense_kernel, len(late), offsets),
        out_shape=jax.ShapeDtypeStruct(hidden.shape, F32),
        in_specs=[in_vmem()] * (2 + len(late) + len(sources)),
        out_specs=in_vmem(),
        compiler_params=params(8),
        cost_estimate=cost(1 << 28, 2 << 20),
        name="dense",
    )(hidden, early, *late, *sources)


def dense_weights(dense_gate, dense_up, dense_down):
    share = dense_gate.shape[1] // lax.axis_size("tp")
    offset = lax.axis_index("tp") * share
    gate = lax.dynamic_slice_in_dim(dense_gate, offset, share, 1)
    up = lax.dynamic_slice_in_dim(dense_up, offset, share, 1)
    down = lax.dynamic_slice_in_dim(dense_down, offset, share, 0)
    return jnp.concatenate(
        [gate.reshape(-1, LANES), up.reshape(-1, LANES), down.reshape(-1, LANES)]
    )


def dense_narrow(hidden, packed, rows, share):
    count = lax.axis_size("ep")
    packed = packed[None]
    bits = [count >> (n + 1) for n in range(count.bit_length() - 1)]
    for bit in bits:
        packed = jnp.concatenate([packed, swap_far(packed, bit)])
    order = [0] * count
    for j in range(count):
        order[sum(bit for n, bit in enumerate(bits) if j >> n & 1)] = j
    packed = jnp.take(packed[jnp.array(order)], lax.axis_index("ep") ^ jnp.arange(count), axis=0)
    packed = packed.reshape(count, 3, rows * share)
    gate = packed[:, 0].reshape(count * rows, share)
    up = packed[:, 1].reshape(count * rows, share)
    down = jnp.moveaxis(packed[:, 2].reshape(count, share, rows), 0, 1).reshape(share, -1)
    act = (jax.nn.silu(dot(hidden, gate)) * dot(hidden, up)).astype(BF16)
    return dot(act, down)


def shards(
    tokens,
    cache_keys,
    cache_values,
    cache_lengths,
    norm_in,
    w_query,
    w_key,
    w_value,
    stick_bias,
    w_output,
    norm_mid,
    routes,
    route_weights,
    expert_gate,
    expert_up,
    expert_down,
    dense_gate,
    dense_up,
    dense_down,
    mix_gate,
    norm_out,
):
    sequences, topk = routes.shape
    ep_count = lax.axis_size("ep")
    experts = ep_count * expert_gate.shape[0]
    capacity = max(2, (sequences * topk + ep_count - 1) // ep_count)
    slots = experts * capacity
    rows = dense_gate.shape[0]
    share = dense_gate.shape[1] // lax.axis_size("tp")
    wide = rows == LANES and share == LANES
    if wide:
        block = pack(dense_gate, dense_up, dense_down)
        columns = [0]
        bit = ep_count // 2
        far = []
        while bit > 2:
            far.append(swap_far(block, bit))
            columns = columns + [c ^ bit for c in columns]
            if bit > 4 or bit == 4:
                block = join(block, far[-1])
            bit //= 2
    partial, normed, place, portion = attention(
        tokens,
        norm_in,
        w_query,
        cache_keys,
        cache_values,
        cache_lengths,
        stick_bias,
        w_output,
        routes,
        route_weights,
        slots,
        capacity,
    )
    partial_other = swap_core(partial)
    hidden, outgoing = middle(partial, partial_other, normed, norm_mid, place)
    received = exchange(outgoing, ep_count)
    received_other = swap_core(received)
    pre, gate, up, down = expert_first(received, expert_gate[0], expert_up[0], expert_down[0])
    sent, act = expert_second(received_other, pre, gate, up, down)
    sent_other = swap_core(sent)
    kept = expert_third(act, down)
    summed = add_rounded(kept, sent_other)
    returned = exchange(summed, ep_count)
    fresh_keys, fresh_values = fresh(normed, w_key, w_value)
    if wide:
        from_x = swap_far(block, 1)
        from_y = swap_far(block, 2)
        part = block.shape[0] // 2
        diagonal_low = swap_far(from_y[:part], 1)
        diagonal_high = swap_far(from_x[part:], 2)
        count = len(columns) // 2
        offsets = (
            tuple(columns),
            tuple(c ^ 1 for c in columns),
            tuple(c ^ 2 for c in columns),
            tuple(c ^ 3 for c in columns[:count]),
            tuple(c ^ 3 for c in columns[count:]),
        )
        pre = dense_early(hidden, (block, from_x, from_y), offsets[:3])
        dense_out = dense(
            hidden,
            pre,
            (diagonal_low, diagonal_high),
            (block, from_x, from_y),
            offsets[3:] + offsets[:3],
        )
    else:
        packed = dense_weights(dense_gate, dense_up, dense_down)
        dense_out = dense_narrow(hidden, packed, rows, share)
    dense_other = swap_core(dense_out)
    own = combine(returned, portion)
    own_other = swap_core(own)
    mixed = last(own, own_other, dense_out, dense_other, hidden, mix_gate, norm_out)
    return (mixed, fresh_keys, fresh_values)


def solution(mesh):
    in_specs = (
        P("ep", None),
        P("ep", "tp", None, None),
        P("ep", "tp", None, None),
        P("ep"),
        P(),
        P(None, "tp"),
        P(None, "tp"),
        P(None, "tp"),
        P("tp"),
        P("tp", None),
        P(),
        P("ep", None),
        P("ep", None),
        P("ep", None, "tp"),
        P("ep", None, "tp"),
        P("ep", "tp", None),
        P("ep", None),
        P("ep", None),
        P(None, "ep"),
        P(),
        P(),
    )
    out_specs = (P("ep", None), P("ep", "tp"), P("ep", "tp"))
    return jax.shard_map(shards, mesh=mesh, in_specs=in_specs, out_specs=out_specs, check_vma=False)
```

```python
import functools

import jax
import jax.numpy as jnp
from jax import lax
from jax.experimental import pallas as pl
from jax.experimental.pallas import tpu as pltpu
from jax.sharding import PartitionSpec as P


LANES = 128
CHUNKS = 2
F32 = jnp.float32
BF16 = jnp.bfloat16
VMEM = pltpu.VMEM
SMEM = pltpu.SMEM
HBM = pltpu.MemorySpace.HBM


def in_vmem():
    return pl.BlockSpec(memory_space=VMEM)


def in_smem():
    return pl.BlockSpec(memory_space=SMEM)


def in_hbm():
    return pl.BlockSpec(memory_space=HBM)


def params(mib):
    return pltpu.CompilerParams(vmem_limit_bytes=mib << 20)


def cost(flops, moved):
    return pl.CostEstimate(flops=flops, bytes_accessed=moved, transcendentals=0)


def iota(shape, dim):
    return lax.broadcasted_iota(jnp.int32, shape, dim)


def dot(a, b):
    return jnp.dot(a, b, preferred_element_type=F32)


def dot_last(a, b):
    return lax.dot_general(a, b, (((1,), (1,)), ((), ())), preferred_element_type=F32)


def dot_first(a, b):
    return lax.dot_general(a, b, (((0,), (0,)), ((), ())), preferred_element_type=F32)


def norm_rows(floats, gain):
    center = jnp.mean(floats, -1, keepdims=True)
    shifted = floats - center
    spread = jnp.mean(jnp.square(shifted), -1, keepdims=True)
    return shifted * lax.rsqrt(spread + 1e-05) * gain


def split_high(values):
    high = values.astype(BF16)
    return high, values - high.astype(F32)


def chunked(src, dst, sems, index):
    size = dst.shape[0] // CHUNKS
    return [
        pltpu.make_async_copy(
            src.at[pl.ds(c * size, size)], dst.at[pl.ds(c * size, size)], sems.at[index, c]
        )
        for c in range(CHUNKS)
    ]


def start_all(copies):
    for copy in copies:
        copy.start()


def wait_all(copies):
    for copy in copies:
        copy.wait()


def plan_slots(capacity, routes, weights, place, share):
    topk, sequences = routes.shape
    slots = place.shape[0]
    expert = iota((slots, sequences), 0) // capacity
    hit = jnp.zeros((slots, sequences), F32)
    weight = jnp.zeros((slots, sequences), F32)
    for j in range(topk):
        match = routes[j : j + 1, :] == expert
        hit = jnp.where(match, 1.0, hit)
        weight = jnp.where(match, weights[j : j + 1, :], weight)
    earlier = (iota((sequences, sequences), 0) < iota((sequences, sequences), 1)).astype(BF16)
    rank = dot(hit.astype(BF16), earlier)
    turn = (iota((slots, sequences), 0) % capacity).astype(F32)
    chosen = (hit > 0.0) & (rank == turn)
    place[...] = jnp.where(chosen, 1.0, 0.0).astype(BF16)
    share[...] = jnp.where(chosen, weight, 0.0)


def attention_kernel(
    capacity,
    lengths,
    bias,
    tokens,
    gain,
    routes,
    weights,
    wq_hbm,
    k_hbm,
    v_hbm,
    wo_hbm,
    partial,
    normed,
    place,
    share,
    wq,
    k,
    v,
    wo,
    sems,
):
    copies = [
        chunked(src, dst, sems, i) for i, (src, dst) in enumerate(((wq_hbm, wq), (k_hbm, k), (v_hbm, v), (wo_hbm, wo)))
    ]
    start_all(copies[0] + copies[1])
    sequences = tokens.shape[0]
    heads = wq.shape[1] * 2 // LANES
    head_dim = LANES // 2
    length = k.shape[1]
    rows = heads * sequences
    wide = sequences * head_dim
    rounded = norm_rows(tokens[...].astype(F32), gain[...]).astype(BF16)
    normed[...] = rounded
    plan_slots(capacity, routes, weights, place, share)
    wait_all(copies[0])
    start_all(copies[2] + copies[3])
    queries = dot(rounded, wq[...]).astype(BF16).astype(F32) * head_dim ** (-0.5)
    low_lane = iota((sequences, LANES), 1) < head_dim
    own_block = iota((sequences, wide), 1) // head_dim == iota((sequences, wide), 0)
    blocks = []
    for h in range(heads):
        slab = queries[:, h // 2 * LANES : (h // 2 + 1) * LANES]
        turned = pltpu.roll(slab, head_dim, 1)
        both = jnp.where(low_lane, slab, turned) if h % 2 == 0 else jnp.where(low_lane, turned, slab)
        blocks.append(jnp.where(own_block, jnp.concatenate([both] * (wide // LANES), axis=1), 0.0))
    spread_queries = jnp.concatenate(blocks, axis=0).astype(BF16)

    row = iota((rows, 1), 0)
    limit = jnp.zeros((rows, 1), jnp.int32)
    for s in range(sequences):
        limit = jnp.where(row % sequences == s, lengths[s], limit)
    offset = jnp.zeros((rows, 1), F32)
    for h in range(heads):
        offset = jnp.where(row // sequences == h, bias[h], offset)
    visible = iota((rows, length), 1) < limit

    wait_all(copies[1])
    scores = dot(spread_queries, k[...]) + offset
    tail = jnp.log1p(jnp.exp(-jnp.abs(scores)))
    keep = jnp.where(visible, -(jnp.maximum(scores, 0.0) + tail), 0.0)
    high, rest = split_high(keep)
    middle, rest = split_high(rest)
    low = rest.astype(BF16)
    span = 2 * LANES
    count = length // span
    pieces = [part[:, n * span : (n + 1) * span] for part in (high, middle, low) for n in range(count)]
    after = (iota((span, span), 0) > iota((span, span), 1)).astype(BF16)
    sums = dot(jnp.concatenate(pieces, axis=0), after)
    carry = jnp.zeros((rows, 1), F32)
    later = [None] * count
    for n in reversed(range(count)):
        within = (
            sums[n * rows : (n + 1) * rows]
            + sums[(count + n) * rows : (count + n + 1) * rows]
            + sums[(2 * count + n) * rows : (2 * count + n + 1) * rows]
        )
        later[n] = within + carry
        carry = carry + within[:, 0:1] + keep[:, n * span : n * span + 1]
    later_sum = jnp.concatenate(later, axis=1)
    stick = jnp.where(visible, jnp.exp(jnp.minimum(scores, 0.0) - tail + later_sum), 0.0).astype(BF16)

    wait_all(copies[2])
    mixed = dot_last(stick, v[...])
    own_rows = iota((rows, wide), 1) // head_dim == iota((rows, wide), 0) % sequences
    mixed = jnp.where(own_rows, mixed, 0.0)
    folded = mixed[:, 0:LANES]
    for j in range(1, wide // LANES):
        folded = folded + mixed[:, j * LANES : (j + 1) * LANES]
    folded = folded + pltpu.roll(folded, head_dim, 1)
    slabs = [
        jnp.where(
            low_lane,
            folded[h * sequences : (h + 1) * sequences],
            folded[(h + 1) * sequences : (h + 2) * sequences],
        )
        for h in range(0, heads, 2)
    ]
    attended = jnp.concatenate(slabs, axis=1).astype(BF16)
    wait_all(copies[3])
    partial[...] = dot(attended, wo[...])


def attention(
    tokens, gain, w_query, keys, values, lengths, bias, w_output, routes, weights, slots, capacity
):
    sequences, kv_local, head_dim, length = keys.shape
    assert kv_local == 1 and head_dim * 2 == LANES
    width = tokens.shape[1]
    wide = sequences * head_dim
    flat = (wide, length)
    return pl.pallas_call(
        functools.partial(attention_kernel, capacity),
        out_shape=(
            jax.ShapeDtypeStruct((sequences, width), F32),
            jax.ShapeDtypeStruct((sequences, width), BF16),
            jax.ShapeDtypeStruct((slots, sequences), BF16),
            jax.ShapeDtypeStruct((slots, sequences), F32),
        ),
        in_specs=[in_smem()] * 2 + [in_vmem()] * 4 + [in_hbm()] * 4,
        out_specs=(in_vmem(),) * 4,
        scratch_shapes=[
            VMEM(w_query.shape, BF16),
            VMEM(flat, BF16),
            VMEM(flat, BF16),
            VMEM(w_output.shape, BF16),
            pltpu.SemaphoreType.DMA((4, CHUNKS)),
        ],
        compiler_params=params(53),
        cost_estimate=cost(1 << 32, 7 << 20),
        name="attention",
    )(
        lengths,
        bias,
        tokens,
        gain.reshape(1, -1),
        jnp.transpose(routes),
        jnp.transpose(weights),
        w_query,
        keys.reshape(flat),
        values.reshape(flat),
        w_output,
    )


def store_rows(scratch, values):
    count, width = values.shape
    parts = width // LANES
    for j in range(parts):
        scratch[pl.ds(j, count, stride=parts), :] = values[:, j * LANES : (j + 1) * LANES]


def load_rows(scratch, count):
    parts = scratch.shape[0] // count
    return jnp.concatenate(
        [scratch[pl.ds(j, count, stride=parts), :] for j in range(parts)], axis=1
    )


def half_of(ref, core, half):
    return ref[:, pl.ds(pl.multiple_of(core * half, half), half)]


def middle_kernel(partial, other, normed, gain, place, hidden, outgoing, scratch):
    half = partial.shape[1] // 2
    floats = normed[...].astype(F32) + (partial[...] + other[...])
    hidden[...] = norm_rows(floats, gain[...]).astype(BF16)
    mine = half_of(hidden, lax.axis_index("tp"), half)
    store_rows(scratch, dot(place[...], mine))
    outgoing[...] = scratch[...].astype(BF16)


def middle(partial, other, normed, gain, place):
    sequences, width = partial.shape
    packed = (place.shape[0] * (width // 2) // LANES, LANES)
    return pl.pallas_call(
        middle_kernel,
        out_shape=(
            jax.ShapeDtypeStruct((sequences, width), BF16),
            jax.ShapeDtypeStruct(packed, BF16),
        ),
        in_specs=[in_vmem()] * 5,
        out_specs=(in_vmem(), in_vmem()),
        scratch_shapes=[VMEM(packed, F32)],
        compiler_params=params(12),
        cost_estimate=cost(1 << 28, 1 << 20),
        name="middle",
    )(partial, other, normed, gain.reshape(1, -1), place)


def first_kernel(own, gate_hbm, up_hbm, down_hbm, pre, gate, up, down, scratch, gate_own, up_own, sems):
    core = lax.axis_index("tp")
    half = gate.shape[0]
    mine = pl.ds(pl.multiple_of(core * half, half), half)
    theirs = pl.ds(pl.multiple_of((1 - core) * half, half), half)
    early = chunked(gate_hbm.at[mine], gate_own, sems, 0) + chunked(up_hbm.at[mine], up_own, sems, 1)
    late = chunked(gate_hbm.at[theirs], gate, sems, 2) + chunked(up_hbm.at[theirs], up, sems, 3)
    late = late + chunked(down_hbm, down, sems, 4)
    start_all(early + late)
    scratch[...] = own[...].astype(F32)
    rows = load_rows(scratch, pre.shape[0]).astype(BF16)
    wait_all(early)
    units = gate.shape[1]
    pre[:, 0:units] = dot(rows, gate_own[...])
    pre[:, units:] = dot(rows, up_own[...])
    wait_all(late)


def expert_first(own, gate, up, down):
    packed = own.shape
    width, units = gate.shape
    half = width // 2
    count = packed[0] * LANES // half
    part = jax.ShapeDtypeStruct((half, units), BF16)
    return pl.pallas_call(
        first_kernel,
        out_shape=(
            jax.ShapeDtypeStruct((count, 2 * units), F32),
            part,
            part,
            jax.ShapeDtypeStruct(down.shape, BF16),
        ),
        in_specs=[in_vmem()] + [in_hbm()] * 3,
        out_specs=(in_vmem(),) * 4,
        scratch_shapes=[
            VMEM(packed, F32),
            VMEM(part.shape, BF16),
            VMEM(part.shape, BF16),
            pltpu.SemaphoreType.DMA((5, CHUNKS)),
        ],
        compiler_params=params(50),
        cost_estimate=cost(1 << 28, 4 << 20),
        name="expert_first",
    )(own, gate, up, down)


def second_kernel(other, pre, gate, up, down, sent, act_out, scratch):
    core = lax.axis_index("tp")
    units = gate.shape[1]
    half = down.shape[1] // 2
    scratch[...] = other[...].astype(F32)
    rows = load_rows(scratch, pre.shape[0]).astype(BF16)
    gate_pre = pre[:, 0:units] + dot(rows, gate[...])
    up_pre = pre[:, units:] + dot(rows, up[...])
    act = (jax.nn.silu(gate_pre) * up_pre).astype(BF16)
    act_out[...] = act
    store_rows(scratch, dot(act, half_of(down, 1 - core, half)))
    sent[...] = scratch[...].astype(BF16)


def expert_second(other, pre, gate, up, down):
    packed = other.shape
    return pl.pallas_call(
        second_kernel,
        out_shape=(
            jax.ShapeDtypeStruct(packed, BF16),
            jax.ShapeDtypeStruct((pre.shape[0], gate.shape[1]), BF16),
        ),
        in_specs=[in_vmem()] * 5,
        out_specs=(in_vmem(), in_vmem()),
        scratch_shapes=[VMEM(packed, F32)],
        compiler_params=params(16),
        cost_estimate=cost(1 << 28, 2 << 20),
        name="expert_second",
    )(other, pre, gate, up, down)


def third_kernel(act, down, kept, scratch):
    half = down.shape[1] // 2
    store_rows(scratch, dot(act[...], half_of(down, lax.axis_index("tp"), half)))
    kept[...] = scratch[...].astype(BF16)


def expert_third(act, down):
    packed = (act.shape[0] * down.shape[1] // 2 // LANES, LANES)
    return pl.pallas_call(
        third_kernel,
        out_shape=jax.ShapeDtypeStruct(packed, BF16),
        in_specs=[in_vmem()] * 2,
        out_specs=in_vmem(),
        scratch_shapes=[VMEM(packed, F32)],
        compiler_params=params(16),
        cost_estimate=cost(1 << 26, 2 << 20),
        name="expert_third",
    )(act, down)


def add_kernel(a, b, out):
    out[...] = (a[...].astype(F32) + b[...].astype(F32)).astype(BF16)


def add_rounded(a, b):
    return pl.pallas_call(
        add_kernel,
        out_shape=jax.ShapeDtypeStruct(a.shape, BF16),
        in_specs=[in_vmem()] * 2,
        out_specs=in_vmem(),
        compiler_params=params(4),
        cost_estimate=cost(1 << 18, 1 << 19),
        name="add_parts",
    )(a, b)


def combine_kernel(returned, share, out, scratch):
    scratch[...] = returned[...].astype(F32)
    rows = load_rows(scratch, share.shape[0]).astype(BF16)
    high, rest = split_high(share[...])
    out[...] = dot_first(high, rows) + dot_first(rest.astype(BF16), rows)


def combine(returned, share):
    half = returned.shape[0] * LANES // share.shape[0]
    return pl.pallas_call(
        combine_kernel,
        out_shape=jax.ShapeDtypeStruct((share.shape[1], half), F32),
        in_specs=[in_vmem()] * 2,
        out_specs=in_vmem(),
        scratch_shapes=[VMEM(returned.shape, F32)],
        compiler_params=params(8),
        cost_estimate=cost(1 << 24, 1 << 19),
        name="combine",
    )(returned, share)


def last_kernel(own, other, dense, dense_other, hidden, mix_gate, gain, mixed, total):
    core = lax.axis_index("tp")
    half = own.shape[1]
    floats = hidden[...].astype(F32)
    mix = jax.nn.sigmoid(jnp.sum(floats * mix_gate[...], axis=-1, keepdims=True))
    total[...] = floats + mix * (dense[...] + dense_other[...])
    mine = pl.ds(pl.multiple_of(core * half, half), half)
    theirs = pl.ds(pl.multiple_of((1 - core) * half, half), half)
    total[:, mine] = total[:, mine] + own[...]
    total[:, theirs] = total[:, theirs] + other[...]
    mixed[...] = norm_rows(total[...], gain[...]).astype(BF16)


def last(own, other, dense, dense_other, hidden, mix_gate, gain):
    return pl.pallas_call(
        last_kernel,
        out_shape=jax.ShapeDtypeStruct(hidden.shape, BF16),
        in_specs=[in_vmem()] * 7,
        out_specs=in_vmem(),
        scratch_shapes=[VMEM(hidden.shape, F32)],
        compiler_params=params(8),
        cost_estimate=cost(1 << 20, 1 << 20),
        name="last",
    )(own, other, dense, dense_other, hidden, mix_gate.reshape(1, -1), gain.reshape(1, -1))


def fresh_kernel(normed, w_key, w_value, keys, values):
    rows = normed[...]
    keys[...] = dot_last(rows, w_key[...]).astype(BF16)
    values[...] = dot_last(rows, w_value[...]).astype(BF16)


def fresh(normed, w_key, w_value):
    shape = jax.ShapeDtypeStruct((normed.shape[0], w_key.shape[1]), BF16)
    return pl.pallas_call(
        fresh_kernel,
        out_shape=(shape, shape),
        in_specs=[in_vmem()] * 3,
        out_specs=(in_vmem(), in_vmem()),
        compiler_params=params(8),
        cost_estimate=cost(1 << 24, 1 << 19),
        name="fresh",
    )(normed, jnp.transpose(w_key), jnp.transpose(w_value))


def swap_core(values):
    return lax.ppermute(values, "tp", [(0, 1), (1, 0)])


def exchange(packed, ep_count):
    blocks = packed.reshape(ep_count, -1, LANES)
    moved = lax.all_to_all(blocks, "ep", split_axis=0, concat_axis=0, tiled=True)
    return moved.reshape(packed.shape)


def swap_far(values, bit):
    count = lax.axis_size("ep")
    return lax.ppermute(values, "ep", [(i, i ^ bit) for i in range(count)])


def pack_kernel(gate_hbm, up_hbm, down_hbm, packed, gate, up, down, sems):
    copies = [
        pltpu.make_async_copy(src, dst, sems.at[i])
        for i, (src, dst) in enumerate(((gate_hbm, gate), (up_hbm, up), (down_hbm, down)))
    ]
    start_all(copies)
    wait_all(copies)
    core = lax.axis_index("tp")
    rows, units = gate.shape
    share = units // 2
    packed[0:rows, 0:share] = half_of(gate, core, share)
    packed[0:rows, share:units] = half_of(up, core, share)
    mine = down[pl.ds(pl.multiple_of(core * share, share), share), :]
    packed[rows:, 0:share] = mine[0 : share // 2]
    packed[rows:, share:units] = mine[share // 2 : share]


def pack(gate, up, down):
    rows, units = gate.shape
    return pl.pallas_call(
        pack_kernel,
        out_shape=jax.ShapeDtypeStruct((rows + units // 4, units), BF16),
        in_specs=[in_hbm()] * 3,
        out_specs=in_vmem(),
        scratch_shapes=[
            VMEM(gate.shape, BF16),
            VMEM(up.shape, BF16),
            VMEM(down.shape, BF16),
            pltpu.SemaphoreType.DMA((3,)),
        ],
        compiler_params=params(63),
        cost_estimate=cost(1 << 32, 1 << 18),
        name="pack",
    )(gate, up, down)


def join_kernel(*refs):
    out, at = refs[-1], 0
    for ref in refs[:-1]:
        out[at : at + ref.shape[0], :] = ref[...]
        at += ref.shape[0]


def join(*blocks):
    rows = sum(block.shape[0] for block in blocks)
    return pl.pallas_call(
        join_kernel,
        out_shape=jax.ShapeDtypeStruct((rows, blocks[0].shape[1]), BF16),
        in_specs=[in_vmem()] * len(blocks),
        out_specs=in_vmem(),
        compiler_params=params(8),
        cost_estimate=cost(1 << 18, 1 << 19),
        name="join",
    )(*blocks)


def slabs_of(sources, offsets):
    height = LANES + sources[0].shape[1] // 4
    me = lax.axis_index("ep")
    return [
        (ref, n * height, pl.ds(pl.multiple_of((me ^ offset) * LANES, LANES), LANES))
        for ref, group in zip(sources, offsets)
        for n, offset in enumerate(group)
    ]


def add_slabs(pre, hidden, slabs):
    for j in range(0, len(slabs), 2):
        left = [hidden[:, at] for _, _, at in slabs[j : j + 2]]
        right = [ref[start : start + LANES, :] for ref, start, _ in slabs[j : j + 2]]
        pre = pre + dot(jnp.concatenate(left, axis=1), jnp.concatenate(right, axis=0))
    return pre


def early_kernel(offsets, hidden, *refs):
    sources, out = refs[:-1], refs[-1]
    out[...] = add_slabs(jnp.zeros(out.shape, F32), hidden, slabs_of(sources, offsets))


def dense_early(hidden, sources, offsets):
    return pl.pallas_call(
        functools.partial(early_kernel, offsets),
        out_shape=jax.ShapeDtypeStruct((hidden.shape[0], sources[0].shape[1]), F32),
        in_specs=[in_vmem()] * (1 + len(sources)),
        out_specs=in_vmem(),
        compiler_params=params(8),
        cost_estimate=cost(1 << 26, 1 << 20),
        name="dense_early",
    )(hidden, *sources)


def dense_kernel(late, offsets, hidden, early, *refs):
    sources, out = refs[:-1], refs[-1]
    share = early.shape[1] // 2
    slabs = slabs_of(sources, offsets)
    count = sum(len(group) for group in offsets[:late])
    pre = add_slabs(early[...], hidden, slabs[:count])
    act = (jax.nn.silu(pre[:, 0:share]) * pre[:, share:]).astype(BF16)
    for j in range(0, len(slabs), 2):
        downs = []
        for ref, start, _ in slabs[j : j + 2]:
            tail = ref[start + LANES : start + LANES + share // 2, :]
            downs.append(jnp.concatenate([tail[:, 0:share], tail[:, share:]], axis=0))
        both = dot(act, jnp.concatenate(downs, axis=1))
        for n, (_, _, at) in enumerate(slabs[j : j + 2]):
            out[:, at] = both[:, n * LANES : (n + 1) * LANES]


def dense(hidden, early, late, sources, offsets):
    return pl.pallas_call(
        functools.partial(dense_kernel, len(late), offsets),
        out_shape=jax.ShapeDtypeStruct(hidden.shape, F32),
        in_specs=[in_vmem()] * (2 + len(late) + len(sources)),
        out_specs=in_vmem(),
        compiler_params=params(8),
        cost_estimate=cost(1 << 28, 2 << 20),
        name="dense",
    )(hidden, early, *late, *sources)


def dense_weights(dense_gate, dense_up, dense_down):
    share = dense_gate.shape[1] // lax.axis_size("tp")
    offset = lax.axis_index("tp") * share
    gate = lax.dynamic_slice_in_dim(dense_gate, offset, share, 1)
    up = lax.dynamic_slice_in_dim(dense_up, offset, share, 1)
    down = lax.dynamic_slice_in_dim(dense_down, offset, share, 0)
    return jnp.concatenate(
        [gate.reshape(-1, LANES), up.reshape(-1, LANES), down.reshape(-1, LANES)]
    )


def dense_narrow(hidden, packed, rows, share):
    count = lax.axis_size("ep")
    packed = packed[None]
    bits = [count >> (n + 1) for n in range(count.bit_length() - 1)]
    for bit in bits:
        packed = jnp.concatenate([packed, swap_far(packed, bit)])
    order = [0] * count
    for j in range(count):
        order[sum(bit for n, bit in enumerate(bits) if j >> n & 1)] = j
    packed = jnp.take(packed[jnp.array(order)], lax.axis_index("ep") ^ jnp.arange(count), axis=0)
    packed = packed.reshape(count, 3, rows * share)
    gate = packed[:, 0].reshape(count * rows, share)
    up = packed[:, 1].reshape(count * rows, share)
    down = jnp.moveaxis(packed[:, 2].reshape(count, share, rows), 0, 1).reshape(share, -1)
    act = (jax.nn.silu(dot(hidden, gate)) * dot(hidden, up)).astype(BF16)
    return dot(act, down)


def shards(
    tokens,
    cache_keys,
    cache_values,
    cache_lengths,
    norm_in,
    w_query,
    w_key,
    w_value,
    stick_bias,
    w_output,
    norm_mid,
    routes,
    route_weights,
    expert_gate,
    expert_up,
    expert_down,
    dense_gate,
    dense_up,
    dense_down,
    mix_gate,
    norm_out,
):
    sequences, topk = routes.shape
    ep_count = lax.axis_size("ep")
    experts = ep_count * expert_gate.shape[0]
    capacity = max(2, (sequences * topk + ep_count - 1) // ep_count)
    slots = experts * capacity
    rows = dense_gate.shape[0]
    share = dense_gate.shape[1] // lax.axis_size("tp")
    wide = rows == LANES and share == LANES
    if wide:
        block = pack(dense_gate, dense_up, dense_down)
        columns = [0]
        bit = ep_count // 2
        far = []
        while bit > 2:
            far.append(swap_far(block, bit))
            columns = columns + [c ^ bit for c in columns]
            if bit > 4 or bit == 4:
                block = join(block, far[-1])
            bit //= 2
    partial, normed, place, portion = attention(
        tokens,
        norm_in,
        w_query,
        cache_keys,
        cache_values,
        cache_lengths,
        stick_bias,
        w_output,
        routes,
        route_weights,
        slots,
        capacity,
    )
    partial_other = swap_core(partial)
    hidden, outgoing = middle(partial, partial_other, normed, norm_mid, place)
    received = exchange(outgoing, ep_count)
    received_other = swap_core(received)
    pre, gate, up, down = expert_first(received, expert_gate[0], expert_up[0], expert_down[0])
    sent, act = expert_second(received_other, pre, gate, up, down)
    sent_other = swap_core(sent)
    kept = expert_third(act, down)
    summed = add_rounded(kept, sent_other)
    returned = exchange(summed, ep_count)
    fresh_keys, fresh_values = fresh(normed, w_key, w_value)
    if wide:
        from_x = swap_far(block, 1)
        from_y = swap_far(block, 2)
        from_d = swap_far(block, 3)
        offsets = (
            tuple(columns),
            tuple(c ^ 1 for c in columns),
            tuple(c ^ 2 for c in columns),
            tuple(c ^ 3 for c in columns),
        )
        pre = dense_early(hidden, (block, from_x, from_y), offsets[:3])
        dense_out = dense(
            hidden,
            pre,
            (from_d,),
            (block, from_x, from_y),
            offsets[3:] + offsets[:3],
        )
    else:
        packed = dense_weights(dense_gate, dense_up, dense_down)
        dense_out = dense_narrow(hidden, packed, rows, share)
    dense_other = swap_core(dense_out)
    own = combine(returned, portion)
    own_other = swap_core(own)
    mixed = last(own, own_other, dense_out, dense_other, hidden, mix_gate, norm_out)
    return (mixed, fresh_keys, fresh_values)


def solution(mesh):
    in_specs = (
        P("ep", None),
        P("ep", "tp", None, None),
        P("ep", "tp", None, None),
        P("ep"),
        P(),
        P(None, "tp"),
        P(None, "tp"),
        P(None, "tp"),
        P("tp"),
        P("tp", None),
        P(),
        P("ep", None),
        P("ep", None),
        P("ep", None, "tp"),
        P("ep", None, "tp"),
        P("ep", "tp", None),
        P("ep", None),
        P("ep", None),
        P(None, "ep"),
        P(),
        P(),
    )
    out_specs = (P("ep", None), P("ep", "tp"), P("ep", "tp"))
    return jax.shard_map(shards, mesh=mesh, in_specs=in_specs, out_specs=out_specs, check_vma=False)
```

```python
import functools

import jax
import jax.numpy as jnp
from jax import lax
from jax.experimental import pallas as pl
from jax.experimental.pallas import tpu as pltpu
from jax.sharding import PartitionSpec as P


LANES = 128
CHUNKS = 2
F32 = jnp.float32
BF16 = jnp.bfloat16
VMEM = pltpu.VMEM
SMEM = pltpu.SMEM
HBM = pltpu.MemorySpace.HBM


def in_vmem():
    return pl.BlockSpec(memory_space=VMEM)


def in_smem():
    return pl.BlockSpec(memory_space=SMEM)


def in_hbm():
    return pl.BlockSpec(memory_space=HBM)


def params(mib):
    return pltpu.CompilerParams(vmem_limit_bytes=mib << 20)


def cost(flops, moved):
    return pl.CostEstimate(flops=flops, bytes_accessed=moved, transcendentals=0)


def iota(shape, dim):
    return lax.broadcasted_iota(jnp.int32, shape, dim)


def dot(a, b):
    return jnp.dot(a, b, preferred_element_type=F32)


def dot_last(a, b):
    return lax.dot_general(a, b, (((1,), (1,)), ((), ())), preferred_element_type=F32)


def dot_first(a, b):
    return lax.dot_general(a, b, (((0,), (0,)), ((), ())), preferred_element_type=F32)


def norm_rows(floats, gain):
    center = jnp.mean(floats, -1, keepdims=True)
    shifted = floats - center
    spread = jnp.mean(jnp.square(shifted), -1, keepdims=True)
    return shifted * lax.rsqrt(spread + 1e-05) * gain


def split_high(values):
    high = values.astype(BF16)
    return high, values - high.astype(F32)


def chunked(src, dst, sems, index):
    size = dst.shape[0] // CHUNKS
    return [
        pltpu.make_async_copy(
            src.at[pl.ds(c * size, size)], dst.at[pl.ds(c * size, size)], sems.at[index, c]
        )
        for c in range(CHUNKS)
    ]


def start_all(copies):
    for copy in copies:
        copy.start()


def wait_all(copies):
    for copy in copies:
        copy.wait()


def plan_slots(capacity, routes, weights, place, share):
    topk, sequences = routes.shape
    slots = place.shape[0]
    expert = iota((slots, sequences), 0) // capacity
    hit = jnp.zeros((slots, sequences), F32)
    weight = jnp.zeros((slots, sequences), F32)
    for j in range(topk):
        match = routes[j : j + 1, :] == expert
        hit = jnp.where(match, 1.0, hit)
        weight = jnp.where(match, weights[j : j + 1, :], weight)
    earlier = (iota((sequences, sequences), 0) < iota((sequences, sequences), 1)).astype(BF16)
    rank = dot(hit.astype(BF16), earlier)
    turn = (iota((slots, sequences), 0) % capacity).astype(F32)
    chosen = (hit > 0.0) & (rank == turn)
    place[...] = jnp.where(chosen, 1.0, 0.0).astype(BF16)
    share[...] = jnp.where(chosen, weight, 0.0)


def attention_kernel(
    capacity,
    lengths,
    bias,
    tokens,
    gain,
    routes,
    weights,
    wq_hbm,
    k_hbm,
    v_hbm,
    wo_hbm,
    partial,
    normed,
    place,
    share,
    wq,
    k,
    v,
    wo,
    sems,
):
    copies = [
        chunked(src, dst, sems, i) for i, (src, dst) in enumerate(((wq_hbm, wq), (k_hbm, k), (v_hbm, v), (wo_hbm, wo)))
    ]
    start_all(copies[0] + copies[1])
    sequences = tokens.shape[0]
    heads = wq.shape[1] * 2 // LANES
    head_dim = LANES // 2
    length = k.shape[1]
    rows = heads * sequences
    wide = sequences * head_dim
    rounded = norm_rows(tokens[...].astype(F32), gain[...]).astype(BF16)
    normed[...] = rounded
    plan_slots(capacity, routes, weights, place, share)
    wait_all(copies[0])
    start_all(copies[2] + copies[3])
    queries = dot(rounded, wq[...]).astype(BF16).astype(F32) * head_dim ** (-0.5)
    low_lane = iota((sequences, LANES), 1) < head_dim
    own_block = iota((sequences, wide), 1) // head_dim == iota((sequences, wide), 0)
    blocks = []
    for h in range(heads):
        slab = queries[:, h // 2 * LANES : (h // 2 + 1) * LANES]
        turned = pltpu.roll(slab, head_dim, 1)
        both = jnp.where(low_lane, slab, turned) if h % 2 == 0 else jnp.where(low_lane, turned, slab)
        blocks.append(jnp.where(own_block, jnp.concatenate([both] * (wide // LANES), axis=1), 0.0))
    spread_queries = jnp.concatenate(blocks, axis=0).astype(BF16)

    row = iota((rows, 1), 0)
    limit = jnp.zeros((rows, 1), jnp.int32)
    for s in range(sequences):
        limit = jnp.where(row % sequences == s, lengths[s], limit)
    offset = jnp.zeros((rows, 1), F32)
    for h in range(heads):
        offset = jnp.where(row // sequences == h, bias[h], offset)
    visible = iota((rows, length), 1) < limit

    wait_all(copies[1])
    scores = dot(spread_queries, k[...]) + offset
    tail = jnp.log1p(jnp.exp(-jnp.abs(scores)))
    keep = jnp.where(visible, -(jnp.maximum(scores, 0.0) + tail), 0.0)
    high, rest = split_high(keep)
    middle, rest = split_high(rest)
    low = rest.astype(BF16)
    span = 2 * LANES
    count = length // span
    pieces = [part[:, n * span : (n + 1) * span] for part in (high, middle, low) for n in range(count)]
    after = (iota((span, span), 0) > iota((span, span), 1)).astype(BF16)
    sums = dot(jnp.concatenate(pieces, axis=0), after)
    carry = jnp.zeros((rows, 1), F32)
    later = [None] * count
    for n in reversed(range(count)):
        within = (
            sums[n * rows : (n + 1) * rows]
            + sums[(count + n) * rows : (count + n + 1) * rows]
            + sums[(2 * count + n) * rows : (2 * count + n + 1) * rows]
        )
        later[n] = within + carry
        carry = carry + within[:, 0:1] + keep[:, n * span : n * span + 1]
    later_sum = jnp.concatenate(later, axis=1)
    stick = jnp.where(visible, jnp.exp(jnp.minimum(scores, 0.0) - tail + later_sum), 0.0).astype(BF16)

    wait_all(copies[2])
    mixed = dot_last(stick, v[...])
    own_rows = iota((rows, wide), 1) // head_dim == iota((rows, wide), 0) % sequences
    mixed = jnp.where(own_rows, mixed, 0.0)
    folded = mixed[:, 0:LANES]
    for j in range(1, wide // LANES):
        folded = folded + mixed[:, j * LANES : (j + 1) * LANES]
    folded = folded + pltpu.roll(folded, head_dim, 1)
    slabs = [
        jnp.where(
            low_lane,
            folded[h * sequences : (h + 1) * sequences],
            folded[(h + 1) * sequences : (h + 2) * sequences],
        )
        for h in range(0, heads, 2)
    ]
    attended = jnp.concatenate(slabs, axis=1).astype(BF16)
    wait_all(copies[3])
    partial[...] = dot(attended, wo[...])


def attention(
    tokens, gain, w_query, keys, values, lengths, bias, w_output, routes, weights, slots, capacity
):
    sequences, kv_local, head_dim, length = keys.shape
    assert kv_local == 1 and head_dim * 2 == LANES
    width = tokens.shape[1]
    wide = sequences * head_dim
    flat = (wide, length)
    return pl.pallas_call(
        functools.partial(attention_kernel, capacity),
        out_shape=(
            jax.ShapeDtypeStruct((sequences, width), F32),
            jax.ShapeDtypeStruct((sequences, width), BF16),
            jax.ShapeDtypeStruct((slots, sequences), BF16),
            jax.ShapeDtypeStruct((slots, sequences), F32),
        ),
        in_specs=[in_smem()] * 2 + [in_vmem()] * 4 + [in_hbm()] * 4,
        out_specs=(in_vmem(),) * 4,
        scratch_shapes=[
            VMEM(w_query.shape, BF16),
            VMEM(flat, BF16),
            VMEM(flat, BF16),
            VMEM(w_output.shape, BF16),
            pltpu.SemaphoreType.DMA((4, CHUNKS)),
        ],
        compiler_params=params(53),
        cost_estimate=cost(1 << 32, 7 << 20),
        name="attention",
    )(
        lengths,
        bias,
        tokens,
        gain.reshape(1, -1),
        jnp.transpose(routes),
        jnp.transpose(weights),
        w_query,
        keys.reshape(flat),
        values.reshape(flat),
        w_output,
    )


def store_rows(scratch, values):
    count, width = values.shape
    parts = width // LANES
    for j in range(parts):
        scratch[pl.ds(j, count, stride=parts), :] = values[:, j * LANES : (j + 1) * LANES]


def load_rows(scratch, count):
    parts = scratch.shape[0] // count
    return jnp.concatenate(
        [scratch[pl.ds(j, count, stride=parts), :] for j in range(parts)], axis=1
    )


def half_of(ref, core, half):
    return ref[:, pl.ds(pl.multiple_of(core * half, half), half)]


def middle_kernel(partial, other, normed, gain, place, hidden, outgoing, scratch):
    half = partial.shape[1] // 2
    floats = normed[...].astype(F32) + (partial[...] + other[...])
    hidden[...] = norm_rows(floats, gain[...]).astype(BF16)
    mine = half_of(hidden, lax.axis_index("tp"), half)
    store_rows(scratch, dot(place[...], mine))
    outgoing[...] = scratch[...].astype(BF16)


def middle(partial, other, normed, gain, place):
    sequences, width = partial.shape
    packed = (place.shape[0] * (width // 2) // LANES, LANES)
    return pl.pallas_call(
        middle_kernel,
        out_shape=(
            jax.ShapeDtypeStruct((sequences, width), BF16),
            jax.ShapeDtypeStruct(packed, BF16),
        ),
        in_specs=[in_vmem()] * 5,
        out_specs=(in_vmem(), in_vmem()),
        scratch_shapes=[VMEM(packed, F32)],
        compiler_params=params(12),
        cost_estimate=cost(1 << 28, 1 << 20),
        name="middle",
    )(partial, other, normed, gain.reshape(1, -1), place)


def first_kernel(own, gate_hbm, up_hbm, down_hbm, pre, gate, up, down, scratch, gate_own, up_own, sems):
    core = lax.axis_index("tp")
    half = gate.shape[0]
    mine = pl.ds(pl.multiple_of(core * half, half), half)
    theirs = pl.ds(pl.multiple_of((1 - core) * half, half), half)
    early = chunked(gate_hbm.at[mine], gate_own, sems, 0) + chunked(up_hbm.at[mine], up_own, sems, 1)
    late = chunked(gate_hbm.at[theirs], gate, sems, 2) + chunked(up_hbm.at[theirs], up, sems, 3)
    late = late + chunked(down_hbm, down, sems, 4)
    start_all(early + late)
    scratch[...] = own[...].astype(F32)
    rows = load_rows(scratch, pre.shape[0]).astype(BF16)
    wait_all(early)
    units = gate.shape[1]
    pre[:, 0:units] = dot(rows, gate_own[...])
    pre[:, units:] = dot(rows, up_own[...])
    wait_all(late)


def expert_first(own, gate, up, down):
    packed = own.shape
    width, units = gate.shape
    half = width // 2
    count = packed[0] * LANES // half
    part = jax.ShapeDtypeStruct((half, units), BF16)
    return pl.pallas_call(
        first_kernel,
        out_shape=(
            jax.ShapeDtypeStruct((count, 2 * units), F32),
            part,
            part,
            jax.ShapeDtypeStruct(down.shape, BF16),
        ),
        in_specs=[in_vmem()] + [in_hbm()] * 3,
        out_specs=(in_vmem(),) * 4,
        scratch_shapes=[
            VMEM(packed, F32),
            VMEM(part.shape, BF16),
            VMEM(part.shape, BF16),
            pltpu.SemaphoreType.DMA((5, CHUNKS)),
        ],
        compiler_params=params(50),
        cost_estimate=cost(1 << 28, 4 << 20),
        name="expert_first",
    )(own, gate, up, down)


def second_kernel(other, pre, gate, up, down, sent, act_out, scratch):
    core = lax.axis_index("tp")
    units = gate.shape[1]
    half = down.shape[1] // 2
    scratch[...] = other[...].astype(F32)
    rows = load_rows(scratch, pre.shape[0]).astype(BF16)
    gate_pre = pre[:, 0:units] + dot(rows, gate[...])
    up_pre = pre[:, units:] + dot(rows, up[...])
    act = (jax.nn.silu(gate_pre) * up_pre).astype(BF16)
    act_out[...] = act
    store_rows(scratch, dot(act, half_of(down, 1 - core, half)))
    sent[...] = scratch[...].astype(BF16)


def expert_second(other, pre, gate, up, down):
    packed = other.shape
    return pl.pallas_call(
        second_kernel,
        out_shape=(
            jax.ShapeDtypeStruct(packed, BF16),
            jax.ShapeDtypeStruct((pre.shape[0], gate.shape[1]), BF16),
        ),
        in_specs=[in_vmem()] * 5,
        out_specs=(in_vmem(), in_vmem()),
        scratch_shapes=[VMEM(packed, F32)],
        compiler_params=params(16),
        cost_estimate=cost(1 << 28, 2 << 20),
        name="expert_second",
    )(other, pre, gate, up, down)


def third_kernel(act, down, kept, scratch):
    half = down.shape[1] // 2
    store_rows(scratch, dot(act[...], half_of(down, lax.axis_index("tp"), half)))
    kept[...] = scratch[...].astype(BF16)


def expert_third(act, down):
    packed = (act.shape[0] * down.shape[1] // 2 // LANES, LANES)
    return pl.pallas_call(
        third_kernel,
        out_shape=jax.ShapeDtypeStruct(packed, BF16),
        in_specs=[in_vmem()] * 2,
        out_specs=in_vmem(),
        scratch_shapes=[VMEM(packed, F32)],
        compiler_params=params(16),
        cost_estimate=cost(1 << 26, 2 << 20),
        name="expert_third",
    )(act, down)


def add_kernel(a, b, out):
    out[...] = (a[...].astype(F32) + b[...].astype(F32)).astype(BF16)


def add_rounded(a, b):
    return pl.pallas_call(
        add_kernel,
        out_shape=jax.ShapeDtypeStruct(a.shape, BF16),
        in_specs=[in_vmem()] * 2,
        out_specs=in_vmem(),
        compiler_params=params(4),
        cost_estimate=cost(1 << 18, 1 << 19),
        name="add_parts",
    )(a, b)


def combine_kernel(returned, share, out, scratch):
    scratch[...] = returned[...].astype(F32)
    rows = load_rows(scratch, share.shape[0]).astype(BF16)
    high, rest = split_high(share[...])
    out[...] = dot_first(high, rows) + dot_first(rest.astype(BF16), rows)


def combine(returned, share):
    half = returned.shape[0] * LANES // share.shape[0]
    return pl.pallas_call(
        combine_kernel,
        out_shape=jax.ShapeDtypeStruct((share.shape[1], half), F32),
        in_specs=[in_vmem()] * 2,
        out_specs=in_vmem(),
        scratch_shapes=[VMEM(returned.shape, F32)],
        compiler_params=params(8),
        cost_estimate=cost(1 << 24, 1 << 19),
        name="combine",
    )(returned, share)


def last_kernel(own, other, dense, dense_other, hidden, mix_gate, gain, mixed, total):
    core = lax.axis_index("tp")
    half = own.shape[1]
    floats = hidden[...].astype(F32)
    mix = jax.nn.sigmoid(jnp.sum(floats * mix_gate[...], axis=-1, keepdims=True))
    total[...] = floats + mix * (dense[...] + dense_other[...])
    mine = pl.ds(pl.multiple_of(core * half, half), half)
    theirs = pl.ds(pl.multiple_of((1 - core) * half, half), half)
    total[:, mine] = total[:, mine] + own[...]
    total[:, theirs] = total[:, theirs] + other[...]
    mixed[...] = norm_rows(total[...], gain[...]).astype(BF16)


def last(own, other, dense, dense_other, hidden, mix_gate, gain):
    return pl.pallas_call(
        last_kernel,
        out_shape=jax.ShapeDtypeStruct(hidden.shape, BF16),
        in_specs=[in_vmem()] * 7,
        out_specs=in_vmem(),
        scratch_shapes=[VMEM(hidden.shape, F32)],
        compiler_params=params(8),
        cost_estimate=cost(1 << 20, 1 << 20),
        name="last",
    )(own, other, dense, dense_other, hidden, mix_gate.reshape(1, -1), gain.reshape(1, -1))


def fresh_kernel(normed, w_key, w_value, keys, values):
    rows = normed[...]
    keys[...] = dot_last(rows, w_key[...]).astype(BF16)
    values[...] = dot_last(rows, w_value[...]).astype(BF16)


def fresh(normed, w_key, w_value):
    shape = jax.ShapeDtypeStruct((normed.shape[0], w_key.shape[1]), BF16)
    return pl.pallas_call(
        fresh_kernel,
        out_shape=(shape, shape),
        in_specs=[in_vmem()] * 3,
        out_specs=(in_vmem(), in_vmem()),
        compiler_params=params(8),
        cost_estimate=cost(1 << 24, 1 << 19),
        name="fresh",
    )(normed, jnp.transpose(w_key), jnp.transpose(w_value))


def swap_core(values):
    return lax.ppermute(values, "tp", [(0, 1), (1, 0)])


def exchange(packed, ep_count):
    blocks = packed.reshape(ep_count, -1, LANES)
    moved = lax.all_to_all(blocks, "ep", split_axis=0, concat_axis=0, tiled=True)
    return moved.reshape(packed.shape)


def swap_far(values, bit):
    count = lax.axis_size("ep")
    return lax.ppermute(values, "ep", [(i, i ^ bit) for i in range(count)])


def pack_kernel(gate_hbm, up_hbm, down_hbm, packed, gate, up, down, sems):
    copies = [
        pltpu.make_async_copy(src, dst, sems.at[i])
        for i, (src, dst) in enumerate(((gate_hbm, gate), (up_hbm, up), (down_hbm, down)))
    ]
    start_all(copies)
    wait_all(copies)
    core = lax.axis_index("tp")
    rows, units = gate.shape
    share = units // 2
    packed[0:rows, 0:share] = half_of(gate, core, share)
    packed[0:rows, share:units] = half_of(up, core, share)
    mine = down[pl.ds(pl.multiple_of(core * share, share), share), :]
    packed[rows:, 0:share] = mine[0 : share // 2]
    packed[rows:, share:units] = mine[share // 2 : share]


def pack(gate, up, down):
    rows, units = gate.shape
    return pl.pallas_call(
        pack_kernel,
        out_shape=jax.ShapeDtypeStruct((rows + units // 4, units), BF16),
        in_specs=[in_hbm()] * 3,
        out_specs=in_vmem(),
        scratch_shapes=[
            VMEM(gate.shape, BF16),
            VMEM(up.shape, BF16),
            VMEM(down.shape, BF16),
            pltpu.SemaphoreType.DMA((3,)),
        ],
        compiler_params=params(63),
        cost_estimate=cost(1 << 32, 1 << 18),
        name="pack",
    )(gate, up, down)


def join_kernel(*refs):
    out, at = refs[-1], 0
    for ref in refs[:-1]:
        out[at : at + ref.shape[0], :] = ref[...]
        at += ref.shape[0]


def join(*blocks):
    rows = sum(block.shape[0] for block in blocks)
    return pl.pallas_call(
        join_kernel,
        out_shape=jax.ShapeDtypeStruct((rows, blocks[0].shape[1]), BF16),
        in_specs=[in_vmem()] * len(blocks),
        out_specs=in_vmem(),
        compiler_params=params(8),
        cost_estimate=cost(1 << 18, 1 << 19),
        name="join",
    )(*blocks)


def slabs_of(sources, offsets):
    height = LANES + sources[0].shape[1] // 4
    me = lax.axis_index("ep")
    return [
        (ref, n * height, pl.ds(pl.multiple_of((me ^ offset) * LANES, LANES), LANES))
        for ref, group in zip(sources, offsets)
        for n, offset in enumerate(group)
    ]


def add_slabs(pre, hidden, slabs):
    for j in range(0, len(slabs), 2):
        left = [hidden[:, at] for _, _, at in slabs[j : j + 2]]
        right = [ref[start : start + LANES, :] for ref, start, _ in slabs[j : j + 2]]
        pre = pre + dot(jnp.concatenate(left, axis=1), jnp.concatenate(right, axis=0))
    return pre


def early_kernel(offsets, hidden, *refs):
    sources, out = refs[:-1], refs[-1]
    out[...] = add_slabs(jnp.zeros(out.shape, F32), hidden, slabs_of(sources, offsets))


def dense_early(hidden, sources, offsets):
    return pl.pallas_call(
        functools.partial(early_kernel, offsets),
        out_shape=jax.ShapeDtypeStruct((hidden.shape[0], sources[0].shape[1]), F32),
        in_specs=[in_vmem()] * (1 + len(sources)),
        out_specs=in_vmem(),
        compiler_params=params(8),
        cost_estimate=cost(1 << 26, 1 << 20),
        name="dense_early",
    )(hidden, *sources)


def dense_kernel(late, offsets, hidden, early, *refs):
    sources, out = refs[:-1], refs[-1]
    share = early.shape[1] // 2
    slabs = slabs_of(sources, offsets)
    count = sum(len(group) for group in offsets[:late])
    pre = add_slabs(early[...], hidden, slabs[:count])
    act = (jax.nn.silu(pre[:, 0:share]) * pre[:, share:]).astype(BF16)
    for j in range(0, len(slabs), 2):
        downs = []
        for ref, start, _ in slabs[j : j + 2]:
            tail = ref[start + LANES : start + LANES + share // 2, :]
            downs.append(jnp.concatenate([tail[:, 0:share], tail[:, share:]], axis=0))
        both = dot(act, jnp.concatenate(downs, axis=1))
        for n, (_, _, at) in enumerate(slabs[j : j + 2]):
            out[:, at] = both[:, n * LANES : (n + 1) * LANES]


def dense(hidden, early, late, sources, offsets):
    return pl.pallas_call(
        functools.partial(dense_kernel, len(late), offsets),
        out_shape=jax.ShapeDtypeStruct(hidden.shape, F32),
        in_specs=[in_vmem()] * (2 + len(late) + len(sources)),
        out_specs=in_vmem(),
        compiler_params=params(8),
        cost_estimate=cost(1 << 28, 2 << 20),
        name="dense",
    )(hidden, early, *late, *sources)


def dense_weights(dense_gate, dense_up, dense_down):
    share = dense_gate.shape[1] // lax.axis_size("tp")
    offset = lax.axis_index("tp") * share
    gate = lax.dynamic_slice_in_dim(dense_gate, offset, share, 1)
    up = lax.dynamic_slice_in_dim(dense_up, offset, share, 1)
    down = lax.dynamic_slice_in_dim(dense_down, offset, share, 0)
    return jnp.concatenate(
        [gate.reshape(-1, LANES), up.reshape(-1, LANES), down.reshape(-1, LANES)]
    )


def dense_narrow(hidden, packed, rows, share):
    count = lax.axis_size("ep")
    packed = packed[None]
    bits = [count >> (n + 1) for n in range(count.bit_length() - 1)]
    for bit in bits:
        packed = jnp.concatenate([packed, swap_far(packed, bit)])
    order = [0] * count
    for j in range(count):
        order[sum(bit for n, bit in enumerate(bits) if j >> n & 1)] = j
    packed = jnp.take(packed[jnp.array(order)], lax.axis_index("ep") ^ jnp.arange(count), axis=0)
    packed = packed.reshape(count, 3, rows * share)
    gate = packed[:, 0].reshape(count * rows, share)
    up = packed[:, 1].reshape(count * rows, share)
    down = jnp.moveaxis(packed[:, 2].reshape(count, share, rows), 0, 1).reshape(share, -1)
    act = (jax.nn.silu(dot(hidden, gate)) * dot(hidden, up)).astype(BF16)
    return dot(act, down)


def shards(
    tokens,
    cache_keys,
    cache_values,
    cache_lengths,
    norm_in,
    w_query,
    w_key,
    w_value,
    stick_bias,
    w_output,
    norm_mid,
    routes,
    route_weights,
    expert_gate,
    expert_up,
    expert_down,
    dense_gate,
    dense_up,
    dense_down,
    mix_gate,
    norm_out,
):
    sequences, topk = routes.shape
    ep_count = lax.axis_size("ep")
    experts = ep_count * expert_gate.shape[0]
    capacity = max(2, (sequences * topk + ep_count - 1) // ep_count)
    slots = experts * capacity
    rows = dense_gate.shape[0]
    share = dense_gate.shape[1] // lax.axis_size("tp")
    wide = rows == LANES and share == LANES and ep_count == 16
    if wide:
        block = pack(dense_gate, dense_up, dense_down)
        far, near = ep_count // 2, ep_count // 4
        block_far = swap_far(block, far)
        block_near = swap_far(block, near)
        block_both = swap_far(block_far, near)
        block = join(block, block_far, block_near, block_both)
        columns = [0, far, near, far + near]
    partial, normed, place, portion = attention(
        tokens,
        norm_in,
        w_query,
        cache_keys,
        cache_values,
        cache_lengths,
        stick_bias,
        w_output,
        routes,
        route_weights,
        slots,
        capacity,
    )
    partial_other = swap_core(partial)
    hidden, outgoing = middle(partial, partial_other, normed, norm_mid, place)
    received = exchange(outgoing, ep_count)
    received_other = swap_core(received)
    pre, gate, up, down = expert_first(received, expert_gate[0], expert_up[0], expert_down[0])
    sent, act = expert_second(received_other, pre, gate, up, down)
    sent_other = swap_core(sent)
    kept = expert_third(act, down)
    summed = add_rounded(kept, sent_other)
    returned = exchange(summed, ep_count)
    fresh_keys, fresh_values = fresh(normed, w_key, w_value)
    if wide:
        from_x = swap_far(block, 1)
        from_y = swap_far(block, 2)
        from_d = swap_far(block, 3)
        offsets = (
            tuple(columns),
            tuple(c ^ 1 for c in columns),
            tuple(c ^ 2 for c in columns),
            tuple(c ^ 3 for c in columns),
        )
        pre = dense_early(hidden, (block, from_x, from_y), offsets[:3])
        dense_out = dense(
            hidden,
            pre,
            (from_d,),
            (block, from_x, from_y),
            offsets[3:] + offsets[:3],
        )
    else:
        packed = dense_weights(dense_gate, dense_up, dense_down)
        dense_out = dense_narrow(hidden, packed, rows, share)
    dense_other = swap_core(dense_out)
    own = combine(returned, portion)
    own_other = swap_core(own)
    mixed = last(own, own_other, dense_out, dense_other, hidden, mix_gate, norm_out)
    return (mixed, fresh_keys, fresh_values)


def solution(mesh):
    in_specs = (
        P("ep", None),
        P("ep", "tp", None, None),
        P("ep", "tp", None, None),
        P("ep"),
        P(),
        P(None, "tp"),
        P(None, "tp"),
        P(None, "tp"),
        P("tp"),
        P("tp", None),
        P(),
        P("ep", None),
        P("ep", None),
        P("ep", None, "tp"),
        P("ep", None, "tp"),
        P("ep", "tp", None),
        P("ep", None),
        P("ep", None),
        P(None, "ep"),
        P(),
        P(),
    )
    out_specs = (P("ep", None), P("ep", "tp"), P("ep", "tp"))
    return jax.shard_map(shards, mesh=mesh, in_specs=in_specs, out_specs=out_specs, check_vma=False)
```
